256 devices in a mesh: sp: 32 (over z, y), fs: 4 (over x), tp: 2 (over core).
Axes of the slice: x: 4, y: 4, z: 8, core: 2. Of those that a mesh axis runs over, the one named last changes fastest.
Arguments:
- tokens: bfloat16 [16384, 2048], P(('fs', 'sp'), 'tp'), parts along dimension 0, may hold values from -6 to 6
- norm_gain: float32 [2048], replicated, may hold values from 0.1 to 1.9
- w_recur_in: bfloat16 [2048, 1024], P(None, 'tp'), may hold values from -0.125 to 0.125
- conv_weight: float32 [4, 1024], P(None, 'tp'), may hold values from -3 to 3
- w_gate_decay: bfloat16 [16, 64, 64], P('tp'), may hold values from -0.75 to 0.75
- w_gate_input: bfloat16 [16, 64, 64], P('tp'), may hold values from -0.75 to 0.75
- decay_base: float32 [1024], P('tp'), may hold values from 0 to 0.01, as said below
- extra_decay: float32 [16384, 16], P(('fs', 'sp'), 'tp'), parts along dimension 0, may hold values from 0 to 1, as said below
- w_query: bfloat16 [2048, 1024], P(None, 'tp'), may hold values from -1 to 1
- w_key: bfloat16 [2048, 256], P(None, 'tp'), may hold values from -20 to 20
- w_value: bfloat16 [2048, 256], P(None, 'tp'), may hold values from -0.125 to 0.125
- mix_lambda: float32 [8], P('tp'), may hold values from 0.3 to 0.8
- head_gain: float32 [128], replicated, may hold values from 0.1 to 1.9
- w_out_recur: bfloat16 [1024, 2048], P('tp'), may hold values from -0.125 to 0.125
- w_out_attend: bfloat16 [1024, 2048], P('tp'), may hold values from -0.125 to 0.125
- out_gain: float32 [2048], replicated, may hold values from 0.1 to 1.9
Outputs:
- mixed: bfloat16 [16384, 2048], P(('fs', 'sp', 'tp')), parts along dimension 0
The draws below stay inside these ranges and needn't reach their ends.
There are 4 independent parts, one for each index of `fs`. The reference program is written for one: setup_inputs(seed, part) draws one part's arguments, and reference() takes and returns one part's arrays. A program takes and returns all parts, laid end to end along the dimension named above; an argument that names none is the same for every part. Nothing has to cross between parts.
Inputs may be any that keep to these rules, and one draw needn't show every extreme that they name: `decay_base`: positive rates of each channel. `extra_decay`: non-negative added log-decays.
All inputs are finite; a program needn't handle non-finite values.
Results may differ from the reference program's by a relative error of at most 0.012.
The reference program's roundings to bfloat16 on the way (of `scaled`, `conv_in`, `recur_out` and `attend_out`) count: a program that leaves them out, or rounds other values in their place, can miss the bound.
Values may be sent and summed in bfloat16 or wider, within the bound.
A program may use at most 128 MiB of HBM per device.

```python
import math
import jax
import jax.numpy as jnp
from jax import lax

D = 2048
HEAD = 64
RECURRENT_HEADS = 16
CONV = 4
DA_HEADS = 8
KV_HEADS = 2
TOK_DEV = 128
RG_W = 1024
DV = 128
SEQUENCE_TOKENS = 4096


def draw_decay_base(key, part):
    slow_key, fast_key, pick_key = jax.random.split(jax.random.fold_in(key, 11), 3)
    slow_rate = jax.random.uniform(slow_key, (RG_W,), jnp.float32, 0.05, 0.15) / SEQUENCE_TOKENS
    fast_rate = jnp.exp(jax.random.uniform(fast_key, (RG_W,), jnp.float32, math.log(0.0025), math.log(0.0083)))
    fast_share = 0.5
    chosen = jax.random.uniform(pick_key, (RG_W,), jnp.float32) < fast_share
    return jnp.where(chosen, fast_rate, slow_rate).astype(jnp.float32)


def draw_extra_decay(key, part):
    level_key, rough_key, position_random_key, amount_random_key = jax.random.split(jax.random.fold_in(key, 23), 4)
    block_count = SEQUENCE_TOKENS // TOK_DEV
    levels = jnp.exp(jax.random.uniform(level_key, (block_count,), jnp.float32, math.log(0.15), math.log(0.6))) / SEQUENCE_TOKENS
    per_position = jnp.repeat(levels, TOK_DEV)
    rough = jax.random.uniform(rough_key, (SEQUENCE_TOKENS, RECURRENT_HEADS), jnp.float32, 0.5, 1.5)
    baseline_term = per_position[:, None] * rough
    spike_positions = jax.random.randint(position_random_key, (3,), 0, SEQUENCE_TOKENS)
    spike_magnitudes = jax.random.uniform(amount_random_key, (3, RECURRENT_HEADS), jnp.float32, 0.22, 0.51)
    spike_marks = (jnp.arange(SEQUENCE_TOKENS)[:, None] == spike_positions[None, :]).astype(jnp.float32)
    spike_values = jnp.dot(spike_marks, spike_magnitudes)
    return (baseline_term + spike_values).astype(jnp.float32)


def query_key_pair(key):
    query_seed, key_seed = jax.random.split(jax.random.fold_in(key, 37))
    spread = 1.3 / math.sqrt(D)
    query_weight = jnp.clip(jax.random.normal(query_seed, (D, DA_HEADS * 2 * HEAD), jnp.float32), -6.0, 6.0) * spread
    key_weight = jnp.clip(jax.random.normal(key_seed, (D, KV_HEADS * 2 * HEAD), jnp.float32), -6.0, 6.0) * spread
    return (query_weight, key_weight)


def draw_w_query(key, part):
    return query_key_pair(key)[0].astype(jnp.bfloat16)


def draw_w_key(key, part):
    return query_key_pair(key)[1].astype(jnp.bfloat16)


def block_scale(own_key, dims, shards, low, largest):
    def one(position, shards_of):
        draws = jax.random.uniform(jax.random.fold_in(jax.random.fold_in(own_key, 6), position), (shards_of,), jnp.float32, low / len(shards), largest / len(shards))
        return jnp.repeat(jnp.exp(draws), dims[position] // shards_of).reshape((-1,) + (1,) * (len(dims) - position - 1))

    factor_of = one(*shards[0])
    for cut in shards[1:]:
        factor_of = factor_of * one(*cut)
    return factor_of


def centred(own_key, dims, deviation, reach, shards=(), kind=jnp.bfloat16):
    gain = block_scale(own_key, dims, shards, -0.22, 0.18) if shards else 1.0
    values = jax.random.normal(own_key, dims, jnp.float32) * deviation * gain
    return jnp.minimum(jnp.maximum(values, -reach), reach).astype(kind)


def setup_inputs(seed: int = 0, part: int = 0) -> dict:
    key_of = jax.random.split(jax.random.key(seed), 17)
    own_keys = jax.random.split(jax.random.fold_in(key_of[16], part), 17)
    return {
        "tokens": centred(own_keys[0], (SEQUENCE_TOKENS, D), 1.0, 6.0, ((0, 32), (1, 2))),
        "norm_gain": jnp.clip(1.0 + 0.18 * jax.random.normal(key_of[1], (D,), jnp.float32), 0.1, 1.9),
        "w_recur_in": centred(key_of[2], (D, RG_W), D ** -0.5, 0.125, ((1, 2),)),
        "conv_weight": centred(key_of[3], (CONV, RG_W), CONV ** -0.5, 3.0, ((1, 2),), jnp.float32),
        "w_gate_decay": centred(key_of[4], (RECURRENT_HEADS, HEAD, HEAD), HEAD ** -0.5, 0.75, ((0, 2),)),
        "w_gate_input": centred(key_of[5], (RECURRENT_HEADS, HEAD, HEAD), HEAD ** -0.5, 0.75, ((0, 2),)),
        "decay_base": draw_decay_base(jax.random.fold_in(key_of[16], 71), part),
        "extra_decay": draw_extra_decay(jax.random.fold_in(jax.random.fold_in(key_of[16], part), 71), part),
        "w_query": draw_w_query(jax.random.fold_in(key_of[16], 71), part),
        "w_key": draw_w_key(jax.random.fold_in(key_of[16], 71), part),
        "w_value": centred(key_of[10], (D, KV_HEADS * DV), D ** -0.5, 0.125, ((1, 2),)),
        "mix_lambda": jnp.clip(0.3 + 0.5 * jax.random.uniform(key_of[11], (DA_HEADS,), jnp.float32) ** block_scale(key_of[11], (DA_HEADS,), ((0, 2),), -0.2, 0.2), 0.3, 0.8),
        "head_gain": jnp.clip(1.0 + 0.18 * jax.random.normal(key_of[12], (DV,), jnp.float32), 0.1, 1.9),
        "w_out_recur": centred(key_of[13], (RG_W, D), (RG_W + DA_HEADS * DV) ** -0.5, 0.125, ((0, 2),)),
        "w_out_attend": centred(key_of[14], (DA_HEADS * DV, D), (RG_W + DA_HEADS * DV) ** -0.5, 0.125, ((0, 2),)),
        "out_gain": jnp.clip(1.0 + 0.18 * jax.random.normal(key_of[15], (D,), jnp.float32), 0.1, 1.9),
    }


lru_rate = 8.0
norm_eps = 1e-06

def chain(earlier, later):
    return (earlier[0] * later[0], later[0] * earlier[1] + later[1])

def reference(tokens, norm_gain, w_recur_in, conv_weight, w_gate_decay, w_gate_input, decay_base, extra_decay, w_query, w_key, w_value, mix_lambda, head_gain, w_out_recur, w_out_attend, out_gain):
    flat = tokens.astype(jnp.float32)
    inverse = lax.rsqrt(lax.optimization_barrier(jnp.mean(flat * flat, axis=1, keepdims=True)) + norm_eps)
    scaled = (flat * norm_gain).astype(jnp.bfloat16)

    def project(weight):
        return (jnp.dot(scaled, weight, preferred_element_type=jnp.float32) * inverse).astype(jnp.bfloat16)
    recur_in = project(w_recur_in)
    queries = project(w_query)
    keys = project(w_key)
    values = project(w_value)
    padded = jnp.concatenate([jnp.zeros((CONV - 1, RG_W), jnp.bfloat16), recur_in], axis=0).astype(jnp.float32)
    conv_acc = jnp.zeros((SEQUENCE_TOKENS, RG_W), jnp.float32)
    for offset in range(CONV):
        conv_acc = conv_acc + conv_weight[offset] * padded[offset:offset + SEQUENCE_TOKENS]
    conv_in = conv_acc.astype(jnp.bfloat16)
    blocks = conv_in.astype(jnp.float32).reshape(SEQUENCE_TOKENS, RECURRENT_HEADS, HEAD)
    decay_gate = jax.nn.sigmoid(jnp.einsum('thi,hij->thj', blocks, w_gate_decay.astype(jnp.float32))).reshape(SEQUENCE_TOKENS, RG_W)
    input_gate = jax.nn.sigmoid(jnp.einsum('thi,hij->thj', blocks, w_gate_input.astype(jnp.float32))).reshape(SEQUENCE_TOKENS, RG_W)
    log_decay = -lru_rate * decay_gate * decay_base - jnp.repeat(extra_decay, HEAD, axis=1)
    decay = jnp.exp(log_decay)
    inject = jnp.sqrt(-jnp.expm1(2.0 * log_decay)) * input_gate * conv_in.astype(jnp.float32)
    unused_total, states = lax.associative_scan(chain, (decay, inject), axis=0)
    recur_out = states.astype(jnp.bfloat16)
    group_size = DA_HEADS // KV_HEADS
    query_four = queries.reshape(SEQUENCE_TOKENS, KV_HEADS, group_size, 2, HEAD)
    key_three = keys.reshape(SEQUENCE_TOKENS, KV_HEADS, 2, HEAD).astype(jnp.float32)
    value_three = values.reshape(SEQUENCE_TOKENS, KV_HEADS, DV).astype(jnp.float32)
    block_rows = math.gcd(SEQUENCE_TOKENS, 512)
    positions = jnp.arange(SEQUENCE_TOKENS, dtype=jnp.int32)
    lambdas = mix_lambda.reshape(KV_HEADS, group_size)

    def one_block(index):
        begin = (index * block_rows).astype(jnp.int32)
        query_part = lax.dynamic_slice_in_dim(query_four, begin, block_rows, 0).astype(jnp.float32)
        allowed = (begin + jnp.arange(block_rows, dtype=jnp.int32))[:, None] >= positions[None, :]
        results = []
        for mapping in range(2):
            scores = jnp.einsum('bkgd,tkd->kgbt', query_part[:, :, :, mapping, :], key_three[:, :, mapping, :]) * HEAD ** (-0.5)
            scores = jnp.where(allowed, scores, -jnp.inf)
            peak = lax.optimization_barrier(jnp.max(scores, axis=-1, keepdims=True))
            expo = jnp.exp(scores - peak)
            total = lax.optimization_barrier(jnp.sum(expo, axis=-1))
            rounded = lax.optimization_barrier(expo.astype(jnp.bfloat16)).astype(jnp.float32)
            attend = jnp.einsum('kgbt,tke->bkge', rounded, value_three)
            results.append(attend / jnp.transpose(total, (2, 0, 1))[..., None])
        return results[0] - lambdas[None, :, :, None] * results[1]
    head_out = lax.map(one_block, jnp.arange(SEQUENCE_TOKENS // block_rows, dtype=jnp.int32))
    head_out = head_out.reshape(SEQUENCE_TOKENS, DA_HEADS, DV)
    normed = head_out * lax.rsqrt(lax.optimization_barrier(jnp.mean(head_out * head_out, axis=-1, keepdims=True)) + norm_eps) * head_gain
    attend_out = normed.astype(jnp.bfloat16).reshape(SEQUENCE_TOKENS, DA_HEADS * DV)
    merged = jnp.dot(recur_out, w_out_recur, preferred_element_type=jnp.float32) + jnp.dot(attend_out, w_out_attend, preferred_element_type=jnp.float32)
    final = merged * lax.rsqrt(lax.optimization_barrier(jnp.mean(merged * merged, axis=1, keepdims=True)) + norm_eps) * out_gain
    return final.astype(jnp.bfloat16)
```

```python
import jax
import jax.numpy as jnp
from jax import lax
from jax.experimental import pallas as pl
from jax.experimental.pallas import tpu as pltpu
from jax.sharding import PartitionSpec as P

MESH = pl.DeviceIdType.MESH
BF = jnp.bfloat16
F32 = jnp.float32

D = 2048
HALF = 1024
HEAD = 64
ROWS = 128
ZN = 8
YN = 4
SP = ZN * YN
RATE = 8.0
EPS = 1e-06
FWD = 4
BACK = 3
NSEND = 96


def dot(a, b):
    return jnp.dot(a, b, preferred_element_type=F32)


def minus_expm1(x):
    series = 1.0 + x * (
        1 / 2 + x * (1 / 6 + x * (1 / 24 + x * (1 / 120 + x * (1 / 720 + x * (1 / 5040 + x / 40320)))))
    )
    return jnp.where(x > -0.5, -x * series, 1.0 - jnp.exp(x))


def kernel(
    tok_h, gain_h, wr_h, cw_h, wgd_h, wgi_h, base_h, extra_h, wq_h, wk_h, wv_h, lam_h, hgain_h,
    wor_h, woa_h, ogain_h, out_h,
    tok, gain, wr, cw, wgd, wgi, base, extra, wq, wkv, lam, hgain, wor, woa, ogain,
    scaled, acc, kbuf, vbuf, rin, halo, xext, qt, att, peak, total, gates,
    crow, ctot, decs, states, mbuf, mrecv, outv,
    lsem, ssem, tsem, ksem, vsem, hsem, crsem, ctsem, msem,
):
    sp = lax.axis_index("sp")
    c = lax.axis_index("tp")
    z = sp // YN
    y = sp % YN

    locals_ = []

    def load(src, dst):
        copy = pltpu.make_async_copy(src, dst, lsem.at[len(locals_)])
        locals_.append(copy)
        copy.start()
        return copy

    own_rows = pl.ds(pl.multiple_of(c * HALF, HALF), HALF)
    other_rows = pl.ds(pl.multiple_of((1 - c) * HALF, HALF), HALF)
    l_tok = load(tok_h, tok.at[c])
    l_gain = load(gain_h, gain)
    l_own = [
        load(wk_h.at[own_rows], wkv.at[own_rows, pl.ds(0, 128)]),
        load(wv_h.at[own_rows], wkv.at[own_rows, pl.ds(128, 128)]),
        load(wr_h.at[own_rows], wr.at[own_rows]),
        load(wq_h.at[own_rows], wq.at[own_rows]),
    ]
    l_kv = [
        load(wk_h.at[other_rows], wkv.at[other_rows, pl.ds(0, 128)]),
        load(wv_h.at[other_rows], wkv.at[other_rows, pl.ds(128, 128)]),
    ]
    l_r = load(wr_h.at[other_rows], wr.at[other_rows])
    l_q = load(wq_h.at[other_rows], wq.at[other_rows])
    l_small = [
        load(cw_h, cw), load(wgd_h, wgd), load(wgi_h, wgi), load(base_h, base), load(extra_h, extra),
        load(lam_h, lam), load(hgain_h, hgain), load(ogain_h, ogain),
    ]

    barrier = pltpu.get_barrier_semaphore()
    pl.semaphore_signal(barrier, inc=1, device_id={"tp": 1 - c}, device_id_type=MESH)
    for step in (1, 2, 3):
        pl.semaphore_signal(
            barrier, inc=1, device_id={"sp": z * YN + (y + step) % YN}, device_id_type=MESH
        )
    for step in (1, ZN - 1):
        pl.semaphore_signal(
            barrier, inc=1, device_id={"sp": ((z + step) % ZN) * YN + y}, device_id_type=MESH
        )
    for step in (1, SP - 1):
        pl.semaphore_signal(
            barrier, inc=1, device_id={"sp": (sp + step) % SP}, device_id_type=MESH
        )

    sends = []

    def send(src, dst, rsem, when=None, **target):
        copy = pltpu.make_async_remote_copy(
            src_ref=src, dst_ref=dst, send_sem=ssem.at[len(sends)], recv_sem=rsem,
            device_id=target, device_id_type=MESH,
        )
        sends.append((copy, when))
        if when is None:
            copy.start()
        else:
            pl.when(when)(lambda: copy.start())

    def arrived(dst, rsem, when=None):
        copy = pltpu.make_async_remote_copy(
            src_ref=dst, dst_ref=dst, send_sem=ssem.at[0], recv_sem=rsem,
            device_id={"tp": 1 - c}, device_id_type=MESH,
        )
        if when is None:
            copy.wait_recv()
        else:
            pl.when(when)(lambda: copy.wait_recv())

    up = ((z + 1) % ZN) * YN + y
    down = ((z + ZN - 1) % ZN) * YN + y

    def beside(step):
        return z * YN + (y + step + YN) % YN

    l_tok.wait()
    pl.semaphore_wait(barrier, 8)
    send(tok.at[c], tok.at[c], tsem, tp=1 - c)
    l_wor = load(wor_h, wor)
    l_woa = load(woa_h, woa)

    l_gain.wait()

    def scale_half(half):
        x = tok[half].astype(F32)
        scaled[half] = (x * gain[half]).astype(BF)
        return jnp.sum(x * x, axis=1, keepdims=True)

    squares = scale_half(c)
    for copy in l_own:
        copy.wait()
    acc[:, 0:256] = dot(scaled[c], wkv[own_rows, :])
    acc[:, 256:768] = dot(scaled[c], wr[own_rows, :])
    acc[:, 768:1280] = dot(scaled[c], wq[own_rows, :])

    arrived(tok.at[1 - c], tsem)
    squares = squares + scale_half(1 - c)
    inverse = lax.rsqrt(squares / D + EPS)
    for copy in l_kv:
        copy.wait()
    kv = (acc[:, 0:256] + dot(scaled[1 - c], wkv[other_rows, :])) * inverse
    kbuf[sp] = kv[:, 0:128].astype(BF)
    vbuf[sp] = jnp.transpose(kv[:, 128:256]).astype(BF)

    def slot(row, col):
        return row * YN + col

    def send_block(buf, sem, row, col, to, when):
        s = slot(row, col)
        send(buf.at[s], buf.at[s], sem.at[s], when=when, sp=to)

    has_up = z < ZN - 1
    goes_down = z <= BACK - 1

    def forward_own(buf, sem, col):
        send_block(buf, sem, z, col, up, has_up)
        send_block(buf, sem, z, col, down, goes_down)

    forward_own(vbuf, vsem, y)
    for step in (1, 3, 2):
        send(kbuf.at[sp], kbuf.at[sp], ksem.at[sp], sp=beside(step))
    forward_own(kbuf, ksem, y)

    def plus(buf, sem, d, col):
        row = jnp.maximum(z - d, 0)
        ok = z >= d
        s = slot(row, col)
        arrived(buf.at[s], sem.at[s], ok)
        if d < FWD:
            send_block(buf, sem, row, col, up, ok & has_up)

    def minus(buf, sem, e, col):
        row = (z + e) % ZN
        ok = row <= BACK - 1
        s = slot(row, col)
        arrived(buf.at[s], sem.at[s], ok)
        if e < BACK:
            send_block(buf, sem, row, col, down, ok)

    def row_plus(d):
        return jnp.maximum(z - d, 0), z >= d

    def row_minus(e):
        row = (z + e) % ZN
        return row, (row <= BACK - 1) & (z > row)

    def spread_v(row, ok):
        way = 1 - 2 * (row % 2)
        send_block(vbuf, vsem, row, y, beside(way), ok)
        send_block(vbuf, vsem, row, y, beside(-way), ok)

    def relay_v(row, ok):
        way = 1 - 2 * (row % 2)
        s = slot(row, (y - way + YN) % YN)
        arrived(vbuf.at[s], vsem.at[s], ok)
        send(vbuf.at[s], vbuf.at[s], vsem.at[s], when=ok, sp=beside(way))

    def finish_v(row, ok):
        way = 1 - 2 * (row % 2)
        for col in ((y + way + YN) % YN, (y + 2) % YN):
            s = slot(row, col)
            arrived(vbuf.at[s], vsem.at[s], ok)

    always = z >= 0
    spread_v(z, always)

    l_r.wait()
    recur = ((acc[:, 256:768] + dot(scaled[1 - c], wr[other_rows, :])) * inverse).astype(BF)
    rin[...] = recur
    send(rin.at[pl.ds(ROWS - 16, 16)], halo, hsem, when=sp < SP - 1, sp=(sp + 1) % SP)
    xext[pl.ds(8, ROWS), :] = recur.astype(F32)

    l_q.wait()
    query = ((acc[:, 768:1280] + dot(scaled[1 - c], wq[other_rows, :])) * inverse).astype(BF)
    query = query.astype(F32) * HEAD ** (-0.5)
    qt[...] = jnp.zeros_like(qt)
    for h in range(4):
        turned = jnp.transpose(query[:, h * 128 : (h + 1) * 128]).astype(BF)
        lanes = slice((h % 2) * 128, (h % 2) * 128 + 128)
        qt[h // 2, 0:64, lanes] = turned[0:64]
        qt[2 + h // 2, 64:128, lanes] = turned[64:128]

    for step in (1, 3, 2):
        col = (y + step) % YN
        s = slot(z, col)
        arrived(kbuf.at[s], ksem.at[s])
        forward_own(kbuf, ksem, col)

    plus(vbuf, vsem, 1, y)
    minus(vbuf, vsem, 1, y)
    spread_v(*row_plus(1))
    spread_v(*row_minus(1))
    plus(kbuf, ksem, 1, y)
    minus(kbuf, ksem, 1, y)
    relay_v(z, always)

    for copy in l_small:
        copy.wait()
    arrived(halo, hsem, sp > 0)
    before = halo[8:16, :].astype(F32)
    xext[pl.ds(0, 8), :] = jnp.where(sp > 0, before, 0.0)
    conv = jnp.zeros((ROWS, 512), F32)
    for k in range(4):
        conv = conv + cw[k : k + 1, :] * xext[pl.ds(5 + k, ROWS), :]
    conv = conv.astype(BF)
    gates[...] = jnp.zeros_like(gates)
    for j in range(4):
        for side in range(2):
            rows = slice(side * 64, side * 64 + 64)
            gates[j, rows, side * 64 : side * 64 + 64] = wgd[2 * j + side]
            gates[j, rows, 128 + side * 64 : 128 + side * 64 + 64] = wgi[2 * j + side]
    lane = lax.broadcasted_iota(jnp.int32, (ROWS, 128), 1)
    line = lax.broadcasted_iota(jnp.int32, (ROWS, 128), 0)
    for j in range(4):
        cols = slice(j * 128, j * 128 + 128)
        part = conv[:, cols]
        both = dot(part, gates[j])
        decay_gate = jax.nn.sigmoid(both[:, 0:128])
        input_gate = jax.nn.sigmoid(both[:, 128:256])
        added = jnp.where(lane < 64, extra[:, 2 * j : 2 * j + 1], extra[:, 2 * j + 1 : 2 * j + 2])
        log_decay = -RATE * decay_gate * base[:, cols] - added
        a = jnp.exp(log_decay)
        b = jnp.sqrt(minus_expm1(2.0 * log_decay)) * input_gate * part.astype(F32)
        for shift in (1, 2, 4, 8, 16, 32, 64):
            inside = line >= shift
            a_back = jnp.where(inside, pltpu.roll(a, shift, 0), 1.0)
            b_back = jnp.where(inside, pltpu.roll(b, shift, 0), 0.0)
            b = a * b_back + b
            a = a * a_back
        decs[:, cols] = a
        states[:, cols] = b
        crow[y, 0:1, cols] = a[ROWS - 1 : ROWS]
        crow[y, 1:2, cols] = b[ROWS - 1 : ROWS]
    for step in (1, 3, 2):
        send(crow.at[y], crow.at[y], crsem.at[y], sp=beside(step))

    def plus_keys(d):
        for step in (1, 3, 2):
            plus(kbuf, ksem, d, (y + step) % YN)

    def minus_keys(e):
        for step in (1, 3, 2):
            minus(kbuf, ksem, e, (y + step) % YN)

    def attend(row, ok, diagonal):
        def all_chunks():
            first = row * YN
            keys = kbuf[pl.ds(first, YN)].reshape(YN * ROWS, 128)
            values = jnp.concatenate([vbuf[first + i] for i in range(YN)], axis=1)

            def one(chunk, carry):
                scores = dot(keys, qt[chunk])
                if diagonal:
                    key_at = lax.broadcasted_iota(jnp.int32, scores.shape, 0)
                    query_at = lax.broadcasted_iota(jnp.int32, scores.shape, 1) % ROWS + y * ROWS
                    scores = jnp.where(query_at >= key_at, scores, -1e30)
                old = peak[chunk]
                new = jnp.maximum(old, jnp.max(scores, axis=0, keepdims=True))
                weights = jnp.exp(scores - new)
                fade = jnp.exp(old - new)
                total[chunk] = total[chunk] * fade + jnp.sum(weights, axis=0, keepdims=True)
                att[chunk] = att[chunk] * fade + dot(values, weights.astype(BF))
                peak[chunk] = new
                return carry

            lax.fori_loop(0, 4, one, 0)

        if ok is None:
            all_chunks()
        else:
            pl.when(ok)(all_chunks)

    plus_keys(1)
    minus_keys(1)
    peak[...] = jnp.full_like(peak, -1e30)
    total[...] = jnp.zeros_like(total)
    att[...] = jnp.zeros_like(att)
    finish_v(z, always)
    attend(z, None, True)

    relay_v(*row_plus(1))
    relay_v(*row_minus(1))
    plus(vbuf, vsem, 2, y)
    minus(vbuf, vsem, 2, y)
    spread_v(*row_plus(2))
    spread_v(*row_minus(2))

    for step in (1, 3, 2):
        col = (y + step) % YN
        arrived(crow.at[col], crsem.at[col])
    all_a = crow[0, 0:1, :]
    all_s = crow[0, 1:2, :]
    for col in range(1, YN):
        all_s = crow[col, 0:1, :] * all_s + crow[col, 1:2, :]
        all_a = crow[col, 0:1, :] * all_a
    ctot[z, 0:1, :] = all_a
    ctot[z, 1:2, :] = all_s
    send(ctot.at[z], ctot.at[z], ctsem.at[z], when=has_up, sp=up)
    send(ctot.at[z], ctot.at[z], ctsem.at[z], when=goes_down, sp=down)

    def plus_carry(d):
        row, ok = row_plus(d)
        arrived(ctot.at[row], ctsem.at[row], ok)
        if d < FWD:
            send(ctot.at[row], ctot.at[row], ctsem.at[row], when=ok & has_up, sp=up)

    def minus_carry(e):
        row = (z + e) % ZN
        ok = row <= BACK - 1
        arrived(ctot.at[row], ctsem.at[row], ok)
        if e < BACK:
            send(ctot.at[row], ctot.at[row], ctsem.at[row], when=ok, sp=down)

    plus(kbuf, ksem, 2, y)
    minus(kbuf, ksem, 2, y)
    plus_keys(2)
    minus_keys(2)
    finish_v(*row_plus(1))
    finish_v(*row_minus(1))
    attend(*row_plus(1), False)
    plus_carry(1)
    minus_carry(1)
    relay_v(*row_plus(2))
    relay_v(*row_minus(2))
    plus(vbuf, vsem, 3, y)
    minus(vbuf, vsem, 3, y)
    spread_v(*row_plus(3))
    spread_v(*row_minus(3))
    plus(kbuf, ksem, 3, y)
    minus(kbuf, ksem, 3, y)
    attend(*row_minus(1), False)
    plus_carry(2)
    minus_carry(2)
    plus_keys(3)
    minus_keys(3)
    finish_v(*row_plus(2))
    finish_v(*row_minus(2))
    attend(*row_plus(2), False)
    plus_carry(3)
    minus_carry(3)
    relay_v(*row_plus(3))
    relay_v(*row_minus(3))
    plus(vbuf, vsem, 4, y)
    spread_v(*row_plus(4))
    plus(kbuf, ksem, 4, y)
    attend(*row_minus(2), False)
    plus_carry(4)

    def fold_total(row, s):
        return ctot[row, 0:1, :] * s + ctot[row, 1:2, :]

    def fold_row(col, s):
        return crow[col, 0:1, :] * s + crow[col, 1:2, :]

    carry_in = lax.fori_loop(0, z, fold_total, jnp.zeros((1, 512), F32))
    carry_in = lax.fori_loop(0, y, fold_row, carry_in)
    recur_out = (states[...] + decs[...] * carry_in).astype(BF)
    l_wor.wait()
    for n in range(4):
        mbuf[n] = dot(recur_out, wor[:, n * 512 : n * 512 + 512])

    finish_v(*row_plus(3))
    finish_v(*row_minus(3))
    attend(*row_plus(3), False)
    relay_v(*row_plus(4))
    attend(*row_minus(3), False)
    plus_keys(4)
    finish_v(*row_plus(4))
    attend(*row_plus(4), False)

    pieces = []
    for h in range(4):
        lanes = slice((h % 2) * 128, (h % 2) * 128 + 128)
        first = att[h // 2, :, lanes] / total[h // 2, :, lanes]
        second = att[2 + h // 2, :, lanes] / total[2 + h // 2, :, lanes]
        out = first - lam[0:1, h : h + 1] * second
        out = out * lax.rsqrt(jnp.mean(out * out, axis=0, keepdims=True) + EPS)
        pieces.append((jnp.transpose(out) * hgain[...]).astype(BF))
    attend_out = jnp.concatenate(pieces, axis=1)

    mine = pl.ds(pl.multiple_of(c * 64, 64), 64)
    theirs = pl.ds(pl.multiple_of((1 - c) * 64, 64), 64)
    l_woa.wait()
    for n in range(4):
        mbuf[n] += dot(attend_out, woa[:, n * 512 : n * 512 + 512])
        send(mbuf.at[n, theirs], mrecv.at[n], msem.at[n], tp=1 - c)
    power = jnp.zeros((64, 1), F32)
    for n in range(4):
        arrived(mrecv.at[n], msem.at[n])
        whole = mbuf[n, mine, :] + mrecv[n]
        mrecv[n] = whole
        power = power + jnp.sum(whole * whole, axis=1, keepdims=True)
    scale = lax.rsqrt(power / D + EPS)
    for n in range(4):
        cols = slice(n * 512, n * 512 + 512)
        outv[:, cols] = (mrecv[n] * scale * ogain[:, cols]).astype(BF)
    last = load(outv, out_h)
    for copy, when in sends:
        if when is None:
            copy.wait_send()
        else:
            pl.when(when)(lambda copy=copy: copy.wait_send())
    last.wait()


def body(
    tokens, norm_gain, w_recur_in, conv_weight, w_gate_decay, w_gate_input, decay_base, extra_decay,
    w_query, w_key, w_value, mix_lambda, head_gain, w_out_recur, w_out_attend, out_gain,
):
    any_ = pl.BlockSpec(memory_space=pl.ANY)
    vmem = pltpu.VMEM
    dma = pltpu.SemaphoreType.DMA
    scratch = [
        vmem((2, ROWS, HALF), BF), vmem((2, 1, HALF), F32), vmem((D, 512), BF), vmem((4, 512), F32),
        vmem((8, 64, 64), BF), vmem((8, 64, 64), BF), vmem((1, 512), F32), vmem((ROWS, 8), F32),
        vmem((D, 512), BF), vmem((D, 256), BF), vmem((1, 4), F32), vmem((1, 128), F32),
        vmem((512, D), BF), vmem((512, D), BF), vmem((1, D), F32),
        vmem((2, ROWS, HALF), BF), vmem((ROWS, 1280), F32),
        vmem((SP, ROWS, 128), BF), vmem((SP, 128, ROWS), BF),
        vmem((ROWS, 512), BF), vmem((16, 512), BF), vmem((ROWS + 8, 512), F32),
        vmem((4, 128, 256), BF), vmem((4, 128, 256), F32), vmem((4, 1, 256), F32), vmem((4, 1, 256), F32),
        vmem((4, 128, 256), BF),
        vmem((YN, 2, 512), F32), vmem((ZN, 2, 512), F32), vmem((ROWS, 512), F32), vmem((ROWS, 512), F32),
        vmem((4, ROWS, 512), F32), vmem((4, 64, 512), F32), vmem((64, D), BF),
        dma((24,)), dma((NSEND,)), dma, dma((SP,)), dma((SP,)), dma, dma((YN,)), dma((ZN,)), dma((4,)),
    ]
    return pl.pallas_call(
        kernel,
        out_shape=jax.ShapeDtypeStruct((64, D), BF),
        in_specs=[any_] * 16,
        out_specs=any_,
        scratch_shapes=scratch,
        compiler_params=pltpu.CompilerParams(
            collective_id=0, has_side_effects=True, vmem_limit_bytes=60 * 1024 * 1024
        ),
        name="layer",
    )(
        tokens, norm_gain.reshape(2, 1, HALF), w_recur_in, conv_weight, w_gate_decay, w_gate_input,
        decay_base.reshape(1, -1), extra_decay, w_query, w_key, w_value, mix_lambda.reshape(1, -1),
        head_gain.reshape(1, -1), w_out_recur, w_out_attend, out_gain.reshape(1, -1),
    )


def solution(mesh):
    in_specs = (
        P(("fs", "sp"), "tp"),
        P(),
        P(None, "tp"),
        P(None, "tp"),
        P("tp", None, None),
        P("tp", None, None),
        P("tp"),
        P(("fs", "sp"), "tp"),
        P(None, "tp"),
        P(None, "tp"),
        P(None, "tp"),
        P("tp"),
        P(),
        P("tp", None),
        P("tp", None),
        P(),
    )
    out_specs = P(("fs", "sp", "tp"), None)
    return jax.shard_map(body, mesh=mesh, in_specs=in_specs, out_specs=out_specs, check_vma=False)
```

```python
import jax
import jax.numpy as jnp
from jax import lax
from jax.experimental import pallas as pl
from jax.experimental.pallas import tpu as pltpu
from jax.sharding import PartitionSpec as P

MESH = pl.DeviceIdType.MESH
BF = jnp.bfloat16
F32 = jnp.float32

D = 2048
HALF = 1024
HEAD = 64
ROWS = 128
ZN = 8
YN = 4
SP = ZN * YN
RATE = 8.0
EPS = 1e-06
FWD = 4
BACK = 3
NSEND = 144


def dot(a, b):
    return jnp.dot(a, b, preferred_element_type=F32)


def minus_expm1(x):
    series = 1.0 + x * (
        1 / 2 + x * (1 / 6 + x * (1 / 24 + x * (1 / 120 + x * (1 / 720 + x * (1 / 5040 + x / 40320)))))
    )
    return jnp.where(x > -0.5, -x * series, 1.0 - jnp.exp(x))


def kernel(
    tok_h, gain_h, wr_h, cw_h, wgd_h, wgi_h, base_h, extra_h, wq_h, wk_h, wv_h, lam_h, hgain_h,
    wor_h, woa_h, ogain_h, out_h,
    tok, gain, wr, cw, wgd, wgi, base, extra, wq, wkv, lam, hgain, wor, woa, ogain,
    scaled, acc, kbuf, vbuf, rin, halo, xext, qt, att, peak, total, gates,
    crow, ctot, decs, states, mbuf, mrecv, rout,
    lsem, ssem, tsem, ksem, vsem, hsem, crsem, ctsem, msem, insem,
):
    sp = lax.axis_index("sp")
    c = lax.axis_index("tp")
    z = sp // YN
    y = sp % YN

    locals_ = []

    def load(src, dst):
        copy = pltpu.make_async_copy(src, dst, lsem.at[len(locals_)])
        locals_.append(copy)
        copy.start()
        return copy

    own_rows = pl.ds(pl.multiple_of(c * HALF, HALF), HALF)
    other_rows = pl.ds(pl.multiple_of((1 - c) * HALF, HALF), HALF)
    l_tok = load(tok_h, tok.at[c])
    l_gain = load(gain_h, gain)
    l_own = [
        load(wk_h.at[own_rows], wkv.at[own_rows, pl.ds(0, 128)]),
        load(wv_h.at[own_rows], wkv.at[own_rows, pl.ds(128, 128)]),
        load(wr_h.at[own_rows], wr.at[own_rows]),
        load(wq_h.at[own_rows], wq.at[own_rows]),
    ]
    l_kv = [
        load(wk_h.at[other_rows], wkv.at[other_rows, pl.ds(0, 128)]),
        load(wv_h.at[other_rows], wkv.at[other_rows, pl.ds(128, 128)]),
    ]
    l_r = load(wr_h.at[other_rows], wr.at[other_rows])
    l_q = load(wq_h.at[other_rows], wq.at[other_rows])
    l_small = [
        load(cw_h, cw), load(wgd_h, wgd), load(wgi_h, wgi), load(base_h, base), load(extra_h, extra),
        load(lam_h, lam), load(hgain_h, hgain), load(ogain_h, ogain),
    ]

    barrier = pltpu.get_barrier_semaphore()
    pl.semaphore_signal(barrier, inc=1, device_id={"tp": 1 - c}, device_id_type=MESH)
    for step in (1, 2, 3):
        pl.semaphore_signal(
            barrier, inc=1, device_id={"sp": z * YN + (y + step) % YN}, device_id_type=MESH
        )
    has_up = z < ZN - 1
    has_down = z > 0
    corner_up = (y == YN - 1) & has_up
    corner_down = (y == 0) & has_down
    greeted = 4
    for when, target in (
        (has_up, (z + 1) * YN + y), (has_down, (z - 1) * YN + y), (corner_up, sp + 1), (corner_down, sp - 1)
    ):
        near = jnp.where(when, target, sp)

        @pl.when(when)
        def _():
            pl.semaphore_signal(barrier, inc=1, device_id={"sp": near}, device_id_type=MESH)

        greeted = greeted + when.astype(jnp.int32)

    sends = []

    def send(src, dst, rsem, when=None, **target):
        copy = pltpu.make_async_remote_copy(
            src_ref=src, dst_ref=dst, send_sem=ssem.at[len(sends)], recv_sem=rsem,
            device_id=target, device_id_type=MESH,
        )
        sends.append((copy, when))
        if when is None:
            copy.start()
        else:
            pl.when(when)(lambda: copy.start())

    def arrived(dst, rsem, when=None):
        copy = pltpu.make_async_remote_copy(
            src_ref=dst, dst_ref=dst, send_sem=ssem.at[0], recv_sem=rsem,
            device_id={"tp": 1 - c}, device_id_type=MESH,
        )
        if when is None:
            copy.wait_recv()
        else:
            pl.when(when)(lambda: copy.wait_recv())

    up = ((z + 1) % ZN) * YN + y
    down = ((z + ZN - 1) % ZN) * YN + y

    def pass_in(k):
        @pl.when(z == ZN - 1 - k)
        def _():
            if k > 0:
                pl.semaphore_wait(insem, 1)
            if k < ZN - 1:
                pl.semaphore_signal(insem, inc=1, device_id={"sp": down}, device_id_type=MESH)

    def beside(step):
        return z * YN + (y + step + YN) % YN

    l_tok.wait()
    pl.semaphore_wait(barrier, greeted)
    send(tok.at[c], tok.at[c], tsem, tp=1 - c)
    pass_in(0)
    l_wor = load(wor_h, wor)
    l_woa = load(woa_h, woa)

    l_gain.wait()

    def scale_half(half):
        x = tok[half].astype(F32)
        scaled[half] = (x * gain[half]).astype(BF)
        return jnp.sum(x * x, axis=1, keepdims=True)

    squares = scale_half(c)
    for copy in l_own:
        copy.wait()
    acc[:, 0:256] = dot(scaled[c], wkv[own_rows, :])
    acc[:, 256:768] = dot(scaled[c], wr[own_rows, :])
    acc[:, 768:1280] = dot(scaled[c], wq[own_rows, :])

    arrived(tok.at[1 - c], tsem)
    squares = squares + scale_half(1 - c)
    inverse = lax.rsqrt(squares / D + EPS)
    for copy in l_kv:
        copy.wait()
    kv = (acc[:, 0:256] + dot(scaled[1 - c], wkv[other_rows, :])) * inverse
    kbuf[sp] = kv[:, 0:128].astype(BF)
    vbuf[sp] = jnp.transpose(kv[:, 128:256]).astype(BF)

    def slot(row, col):
        return row * YN + col

    def send_block(buf, sem, row, col, to, when):
        s = slot(row, col)
        send(buf.at[s], buf.at[s], sem.at[s], when=when, sp=to)

    goes_down = z <= BACK - 1
    postponed = []

    def send_down(buf, sem, at, when):
        send(buf.at[at], buf.at[at], sem.at[at], when=when & has_down, sp=down)
        wrap = lambda: send(buf.at[at], buf.at[at], sem.at[at], when=when & (z == 0), sp=down)
        if postponed is None:
            wrap()
        else:
            postponed.append(wrap)

    def forward_own(buf, sem, col):
        send_block(buf, sem, z, col, up, has_up)
        send_down(buf, sem, slot(z, col), goes_down)

    forward_own(vbuf, vsem, y)
    for step in (1, 3, 2):
        send(kbuf.at[sp], kbuf.at[sp], ksem.at[sp], sp=beside(step))
    forward_own(kbuf, ksem, y)

    def plus(buf, sem, d, col):
        row = jnp.maximum(z - d, 0)
        ok = z >= d
        s = slot(row, col)
        arrived(buf.at[s], sem.at[s], ok)
        if d < FWD:
            send_block(buf, sem, row, col, up, ok & has_up)

    def minus(buf, sem, e, col):
        row = (z + e) % ZN
        ok = row <= BACK - 1
        s = slot(row, col)
        arrived(buf.at[s], sem.at[s], ok)
        if e < BACK:
            send_down(buf, sem, s, ok)

    def row_plus(d):
        return jnp.maximum(z - d, 0), z >= d

    def row_minus(e):
        row = (z + e) % ZN
        return row, (row <= BACK - 1) & (z > row)

    def spread_v(row, ok):
        way = 1 - 2 * (row % 2)
        send_block(vbuf, vsem, row, y, beside(way), ok)
        send_block(vbuf, vsem, row, y, beside(-way), ok)

    def relay_v(row, ok):
        way = 1 - 2 * (row % 2)
        s = slot(row, (y - way + YN) % YN)
        arrived(vbuf.at[s], vsem.at[s], ok)
        send(vbuf.at[s], vbuf.at[s], vsem.at[s], when=ok, sp=beside(way))

    def finish_v(row, ok):
        way = 1 - 2 * (row % 2)
        for col in ((y + way + YN) % YN, (y + 2) % YN):
            s = slot(row, col)
            arrived(vbuf.at[s], vsem.at[s], ok)

    always = z >= 0
    spread_v(z, always)

    l_r.wait()
    recur = ((acc[:, 256:768] + dot(scaled[1 - c], wr[other_rows, :])) * inverse).astype(BF)
    rin[...] = recur
    send(rin.at[pl.ds(ROWS - 16, 16)], halo, hsem, when=sp < SP - 1, sp=(sp + 1) % SP)
    xext[pl.ds(8, ROWS), :] = recur.astype(F32)

    pass_in(1)

    def v_plus(d):
        plus(vbuf, vsem, d, y)
        spread_v(*row_plus(d))

    def v_minus(e):
        minus(vbuf, vsem, e, y)
        spread_v(*row_minus(e))

    l_q.wait()
    query = ((acc[:, 768:1280] + dot(scaled[1 - c], wq[other_rows, :])) * inverse).astype(BF)
    query = query.astype(F32) * HEAD ** (-0.5)
    qt[...] = jnp.zeros_like(qt)
    for h in range(4):
        turned = jnp.transpose(query[:, h * 128 : (h + 1) * 128]).astype(BF)
        lanes = slice((h % 2) * 128, (h % 2) * 128 + 128)
        qt[h // 2, 0:64, lanes] = turned[0:64]
        qt[2 + h // 2, 64:128, lanes] = turned[64:128]

    pass_in(2)
    v_plus(1)

    for step in (1, 3, 2):
        col = (y + step) % YN
        s = slot(z, col)
        arrived(kbuf.at[s], ksem.at[s])
        forward_own(kbuf, ksem, col)
    plus(kbuf, ksem, 1, y)
    pass_in(3)
    relay_v(z, always)

    for copy in l_small:
        copy.wait()
    arrived(halo, hsem, sp > 0)
    before = halo[8:16, :].astype(F32)
    xext[pl.ds(0, 8), :] = jnp.where(sp > 0, before, 0.0)
    conv = jnp.zeros((ROWS, 512), F32)
    for k in range(4):
        conv = conv + cw[k : k + 1, :] * xext[pl.ds(5 + k, ROWS), :]
    conv = conv.astype(BF)
    gates[...] = jnp.zeros_like(gates)
    for j in range(4):
        for side in range(2):
            rows = slice(side * 64, side * 64 + 64)
            gates[j, rows, side * 64 : side * 64 + 64] = wgd[2 * j + side]
            gates[j, rows, 128 + side * 64 : 128 + side * 64 + 64] = wgi[2 * j + side]
    lane = lax.broadcasted_iota(jnp.int32, (ROWS, 128), 1)
    line = lax.broadcasted_iota(jnp.int32, (ROWS, 128), 0)
    extra_t = jnp.transpose(extra[...])
    def recur_columns(j):
        cols = slice(j * 128, j * 128 + 128)
        part = conv[:, cols]
        both = dot(part, gates[j])
        decay_gate = jax.nn.sigmoid(both[:, 0:128])
        input_gate = jax.nn.sigmoid(both[:, 128:256])
        added = jnp.where(lane < 64, extra_t[:, 2 * j : 2 * j + 1], extra_t[:, 2 * j + 1 : 2 * j + 2])
        log_decay = -RATE * decay_gate * base[:, cols] - added
        a = jnp.exp(log_decay)
        b = jnp.sqrt(minus_expm1(2.0 * log_decay)) * input_gate * part.astype(F32)
        for shift in (1, 2, 4, 8, 16, 32, 64):
            inside = line >= shift
            a_back = jnp.where(inside, pltpu.roll(a, shift, 0), 1.0)
            b_back = jnp.where(inside, pltpu.roll(b, shift, 0), 0.0)
            b = a * b_back + b
            a = a * a_back
        decs[:, cols] = a
        states[:, cols] = b
        crow[y, 0:1, cols] = a[ROWS - 1 : ROWS]
        crow[y, 1:2, cols] = b[ROWS - 1 : ROWS]

    pass_in(4)
    recur_columns(0)
    v_plus(2)
    v_minus(1)
    pass_in(5)
    recur_columns(1)
    recur_columns(2)
    v_minus(2)
    pass_in(6)
    recur_columns(3)
    for step in (1, 3, 2):
        send(crow.at[y], crow.at[y], crsem.at[y], sp=beside(step))
    pass_in(7)
    for wrap in postponed:
        wrap()
    postponed = None
    relay_v(*row_plus(1))

    def key(sign, n, step):
        move = plus if sign > 0 else minus
        return lambda: move(kbuf, ksem, n, (y + step) % YN)

    def attend(row, ok, part, diagonal=False, steps=None):
        def run():
            if steps is None:
                first = row * YN
                keys = kbuf[pl.ds(first, YN)].reshape(YN * ROWS, 128)
                values = jnp.concatenate([vbuf[first + i] for i in range(YN)], axis=1)
            else:
                slots = [slot(row, (y + step) % YN) for step in steps]
                keys = jnp.concatenate([kbuf[s] for s in slots], axis=0)
                values = jnp.concatenate([vbuf[s] for s in slots], axis=1)
            scores = dot(keys, qt[part])
            if diagonal:
                key_at = lax.broadcasted_iota(jnp.int32, scores.shape, 0)
                query_at = lax.broadcasted_iota(jnp.int32, scores.shape, 1) % ROWS + y * ROWS
                scores = jnp.where(query_at >= key_at, scores, -1e30)
                new = jnp.max(scores, axis=0, keepdims=True)
                weights = jnp.exp(scores - new)
                total[part] = jnp.sum(weights, axis=0, keepdims=True)
                att[part] = dot(values, weights.astype(BF))
            else:
                old = peak[part]
                new = jnp.maximum(old, jnp.max(scores, axis=0, keepdims=True))
                weights = jnp.exp(scores - new)
                fade = jnp.exp(old - new)
                total[part] = total[part] * fade + jnp.sum(weights, axis=0, keepdims=True)
                att[part] = att[part] * fade + dot(values, weights.astype(BF))
            peak[part] = new

        if ok is None:
            run()
        else:
            pl.when(ok)(run)

    fillers = []

    def filler():
        if fillers:
            fillers.pop(0)()

    def ready(row, ok, **how):
        for part in range(4):
            fillers.append(lambda part=part: attend(row, ok, part, **how))

    def run(*ops):
        for op in ops:
            op()
            filler()

    def row_carry():
        for step in (1, 3, 2):
            col = (y + step) % YN
            arrived(crow.at[col], crsem.at[col])
        all_a = crow[0, 0:1, :]
        all_s = crow[0, 1:2, :]
        for col in range(1, YN):
            all_s = crow[col, 0:1, :] * all_s + crow[col, 1:2, :]
            all_a = crow[col, 0:1, :] * all_a
        ctot[z, 0:1, :] = all_a
        ctot[z, 1:2, :] = all_s
        send(ctot.at[z], ctot.at[z], ctsem.at[z], when=has_up, sp=up)
        send_down(ctot, ctsem, z, goes_down)

    def carry(n):
        row, ok = row_plus(n)
        arrived(ctot.at[row], ctsem.at[row], ok)
        if n < FWD:
            send(ctot.at[row], ctot.at[row], ctsem.at[row], when=ok & has_up, sp=up)
        if n <= BACK:
            row = (z + n) % ZN
            ok = row <= BACK - 1
            arrived(ctot.at[row], ctsem.at[row], ok)
            if n < BACK:
                send_down(ctot, ctsem, row, ok)

    def fold_total(row, s):
        return ctot[row, 0:1, :] * s + ctot[row, 1:2, :]

    def fold_row(col, s):
        return crow[col, 0:1, :] * s + crow[col, 1:2, :]

    def recur_output():
        carry_in = lax.fori_loop(0, z, fold_total, jnp.zeros((1, 512), F32))
        carry_in = lax.fori_loop(0, y, fold_row, carry_in)
        rout[...] = (states[...] + decs[...] * carry_in).astype(BF)
        l_wor.wait()

    def recur_project(n):
        mbuf[n] = dot(rout[...], wor[:, n * 512 : n * 512 + 512])

    finish_v(z, always)
    ready(z, None, diagonal=True)
    run(key(1, 1, 1), key(1, 1, 3), key(1, 1, 2))
    run(lambda: v_plus(3), lambda: v_minus(3))
    run(lambda: relay_v(*row_plus(2)), lambda: relay_v(*row_minus(1)), lambda: finish_v(*row_plus(1)))
    ready(*row_plus(1))
    run(key(-1, 1, 0), key(-1, 1, 1), key(1, 2, 0), key(-1, 1, 3), key(1, 2, 1), row_carry)
    run(key(-1, 1, 2), key(1, 2, 3), key(1, 2, 2), lambda: relay_v(*row_minus(2)))
    run(lambda: v_plus(4), lambda: relay_v(*row_plus(3)), lambda: finish_v(*row_plus(2)))
    ready(*row_plus(2))
    run(lambda: finish_v(*row_minus(1)), lambda: relay_v(*row_minus(3)))
    ready(*row_minus(1))
    run(lambda: carry(1), key(-1, 2, 0), key(-1, 2, 1), key(1, 3, 0), key(-1, 2, 3), key(1, 3, 1))
    run(key(-1, 2, 2), key(1, 3, 3), lambda: carry(2), key(1, 3, 2), lambda: finish_v(*row_minus(2)))
    ready(*row_minus(2))
    run(lambda: relay_v(*row_plus(4)), lambda: finish_v(*row_plus(3)), lambda: finish_v(*row_minus(3)))
    ready(*row_plus(3))
    run(lambda: carry(3), key(-1, 3, 0), key(-1, 3, 1), key(-1, 3, 3), lambda: carry(4), key(-1, 3, 2))
    fillers.append(recur_output)
    for n in range(4):
        fillers.append(lambda n=n: recur_project(n))
    ready(*row_minus(3))
    run(lambda: finish_v(*row_plus(4)), key(1, 4, 0), key(1, 4, 1))
    ready(*row_plus(4), steps=(0, 1))
    run(key(1, 4, 3))
    while len(fillers) > 1:
        filler()
    run(key(1, 4, 2))
    ready(*row_plus(4), steps=(3, 2))
    while fillers:
        filler()

    pieces = []
    for h in range(4):
        lanes = slice((h % 2) * 128, (h % 2) * 128 + 128)
        first = att[h // 2, :, lanes] / total[h // 2, :, lanes]
        second = att[2 + h // 2, :, lanes] / total[2 + h // 2, :, lanes]
        out = first - lam[0:1, h : h + 1] * second
        out = out * lax.rsqrt(jnp.mean(out * out, axis=0, keepdims=True) + EPS)
        pieces.append((jnp.transpose(out) * hgain[...]).astype(BF))
    attend_out = jnp.concatenate(pieces, axis=1)

    mine = pl.ds(pl.multiple_of(c * 64, 64), 64)
    theirs = pl.ds(pl.multiple_of((1 - c) * 64, 64), 64)
    l_woa.wait()
    for n in range(4):
        mbuf[n] += dot(attend_out, woa[:, n * 512 : n * 512 + 512])
        send(mbuf.at[n, theirs], mrecv.at[n], msem.at[n], tp=1 - c)
    power = jnp.zeros((64, 1), F32)
    for n in range(4):
        arrived(mrecv.at[n], msem.at[n])
        whole = mbuf[n, mine, :] + mrecv[n]
        mrecv[n] = whole
        power = power + jnp.sum(whole * whole, axis=1, keepdims=True)
    scale = lax.rsqrt(power / D + EPS)
    for n in range(4):
        cols = slice(n * 512, n * 512 + 512)
        out_h[:, cols] = (mrecv[n] * scale * ogain[:, cols]).astype(BF)
    for copy, when in sends:
        if when is None:
            copy.wait_send()
        else:
            pl.when(when)(lambda copy=copy: copy.wait_send())


def body(
    tokens, norm_gain, w_recur_in, conv_weight, w_gate_decay, w_gate_input, decay_base, extra_decay,
    w_query, w_key, w_value, mix_lambda, head_gain, w_out_recur, w_out_attend, out_gain,
):
    any_ = pl.BlockSpec(memory_space=pl.ANY)
    vmem = pltpu.VMEM
    dma = pltpu.SemaphoreType.DMA
    scratch = [
        vmem((2, ROWS, HALF), BF), vmem((2, 1, HALF), F32), vmem((D, 512), BF), vmem((4, 512), F32),
        vmem((8, 64, 64), BF), vmem((8, 64, 64), BF), vmem((1, 512), F32), vmem((8, ROWS), F32),
        vmem((D, 512), BF), vmem((D, 256), BF), vmem((1, 4), F32), vmem((1, 128), F32),
        vmem((512, D), BF), vmem((512, D), BF), vmem((1, D), F32),
        vmem((2, ROWS, HALF), BF), vmem((ROWS, 1280), F32),
        vmem((SP, ROWS, 128), BF), vmem((SP, 128, ROWS), BF),
        vmem((ROWS, 512), BF), vmem((16, 512), BF), vmem((ROWS + 8, 512), F32),
        vmem((4, 128, 256), BF), vmem((4, 128, 256), F32), vmem((4, 1, 256), F32), vmem((4, 1, 256), F32),
        vmem((4, 128, 256), BF),
        vmem((YN, 2, 512), F32), vmem((ZN, 2, 512), F32), vmem((ROWS, 512), F32), vmem((ROWS, 512), F32),
        vmem((4, ROWS, 512), F32), vmem((4, 64, 512), F32), vmem((ROWS, 512), BF),
        dma((24,)), dma((NSEND,)), dma, dma((SP,)), dma((SP,)), dma, dma((YN,)), dma((ZN,)), dma((4,)),
        pltpu.SemaphoreType.REGULAR,
    ]
    return pl.pallas_call(
        kernel,
        out_shape=pltpu.VMEM((64, D), BF),
        in_specs=[any_] * 16,
        out_specs=pl.BlockSpec(memory_space=pltpu.VMEM),
        scratch_shapes=scratch,
        compiler_params=pltpu.CompilerParams(
            collective_id=0, has_side_effects=True, vmem_limit_bytes=60 * 1024 * 1024
        ),
        name="layer",
    )(
        tokens, norm_gain.reshape(2, 1, HALF), w_recur_in, conv_weight, w_gate_decay, w_gate_input,
        decay_base.reshape(1, -1), extra_decay.T, w_query, w_key, w_value, mix_lambda.reshape(1, -1),
        head_gain.reshape(1, -1), w_out_recur, w_out_attend, out_gain.reshape(1, -1),
    )


def solution(mesh):
    in_specs = (
        P(("fs", "sp"), "tp"),
        P(),
        P(None, "tp"),
        P(None, "tp"),
        P("tp", None, None),
        P("tp", None, None),
        P("tp"),
        P(("fs", "sp"), "tp"),
        P(None, "tp"),
        P(None, "tp"),
        P(None, "tp"),
        P("tp"),
        P(),
        P("tp", None),
        P("tp", None),
        P(),
    )
    out_specs = P(("fs", "sp", "tp"), None)
    return jax.shard_map(body, mesh=mesh, in_specs=in_specs, out_specs=out_specs, check_vma=False)
```

```python
import jax
import jax.numpy as jnp
from jax import lax
from jax.experimental import pallas as pl
from jax.experimental.pallas import tpu as pltpu
from jax.sharding import PartitionSpec as P

MESH = pl.DeviceIdType.MESH
BF = jnp.bfloat16
F32 = jnp.float32

D = 2048
HALF = 1024
HEAD = 64
ROWS = 128
ZN = 8
YN = 4
SP = ZN * YN
RATE = 8.0
EPS = 1e-06
FWD = 4
BACK = 3
NSEND = 144


def dot(a, b):
    return jnp.dot(a, b, preferred_element_type=F32)


def minus_expm1(x):
    series = 1.0 + x * (
        1 / 2 + x * (1 / 6 + x * (1 / 24 + x * (1 / 120 + x * (1 / 720 + x * (1 / 5040 + x / 40320)))))
    )
    return jnp.where(x > -0.5, -x * series, 1.0 - jnp.exp(x))


def kernel(
    tok_h, gain_h, wr_h, cw_h, wgd_h, wgi_h, base_h, extra_h, wq_h, wk_h, wv_h, lam_h, hgain_h,
    wor_h, woa_h, ogain_h, out_h,
    tok, gain, wr, cw, wgd, wgi, base, extra, wq, wkv, lam, hgain, wor, woa, ogain,
    scaled, acc, kbuf, vbuf, rin, halo, xext, qt, att, peak, total, gates,
    crow, ctot, decs, states, mbuf, mrecv, rout,
    lsem, ssem, tsem, ksem, vsem, hsem, crsem, ctsem, msem,
):
    sp = lax.axis_index("sp")
    c = lax.axis_index("tp")
    z = sp // YN
    y = sp % YN

    locals_ = []

    def load(src, dst):
        copy = pltpu.make_async_copy(src, dst, lsem.at[len(locals_)])
        locals_.append(copy)
        copy.start()
        return copy

    own_rows = pl.ds(pl.multiple_of(c * HALF, HALF), HALF)
    other_rows = pl.ds(pl.multiple_of((1 - c) * HALF, HALF), HALF)
    l_tok = load(tok_h, tok.at[c])
    l_gain = load(gain_h, gain)
    l_own = [
        load(wk_h.at[own_rows], wkv.at[own_rows, pl.ds(0, 128)]),
        load(wv_h.at[own_rows], wkv.at[own_rows, pl.ds(128, 128)]),
        load(wr_h.at[own_rows], wr.at[own_rows]),
        load(wq_h.at[own_rows], wq.at[own_rows]),
    ]
    l_kv = [
        load(wk_h.at[other_rows], wkv.at[other_rows, pl.ds(0, 128)]),
        load(wv_h.at[other_rows], wkv.at[other_rows, pl.ds(128, 128)]),
    ]
    l_r = load(wr_h.at[other_rows], wr.at[other_rows])
    l_q = load(wq_h.at[other_rows], wq.at[other_rows])
    l_small = [
        load(cw_h, cw), load(wgd_h, wgd), load(wgi_h, wgi), load(base_h, base), load(extra_h, extra),
        load(lam_h, lam), load(hgain_h, hgain), load(ogain_h, ogain),
    ]

    barrier = pltpu.get_barrier_semaphore()
    pl.semaphore_signal(barrier, inc=1, device_id={"tp": 1 - c}, device_id_type=MESH)
    for step in (1, 2, 3):
        pl.semaphore_signal(
            barrier, inc=1, device_id={"sp": z * YN + (y + step) % YN}, device_id_type=MESH
        )
    has_up = z < ZN - 1
    has_down = z > 0
    around = (z == 0) | (z == ZN - 1)
    corner_up = (y == YN - 1) & has_up
    corner_down = (y == 0) & has_down
    greeted = 4
    for when, target in (
        (has_up, (z + 1) * YN + y), (has_down, (z - 1) * YN + y), (around, (ZN - 1 - z) * YN + y),
        (corner_up, sp + 1), (corner_down, sp - 1),
    ):
        near = jnp.where(when, target, sp)

        @pl.when(when)
        def _():
            pl.semaphore_signal(barrier, inc=1, device_id={"sp": near}, device_id_type=MESH)

        greeted = greeted + when.astype(jnp.int32)

    sends = []
    numbers = iter(range(NSEND))

    def send(src, dst, rsem, when=None, **target):
        copy = pltpu.make_async_remote_copy(
            src_ref=src, dst_ref=dst, send_sem=ssem.at[next(numbers)], recv_sem=rsem,
            device_id=target, device_id_type=MESH,
        )
        sends.append((copy, when))
        if when is None:
            copy.start()
        else:
            pl.when(when)(lambda: copy.start())

    def arrived(dst, rsem, when=None):
        copy = pltpu.make_async_remote_copy(
            src_ref=dst, dst_ref=dst, send_sem=ssem.at[0], recv_sem=rsem,
            device_id={"tp": 1 - c}, device_id_type=MESH,
        )
        if when is None:
            copy.wait_recv()
        else:
            pl.when(when)(lambda: copy.wait_recv())

    up = ((z + 1) % ZN) * YN + y
    down = ((z + ZN - 1) % ZN) * YN + y

    def beside(step):
        return z * YN + (y + step + YN) % YN

    l_tok.wait()
    pl.semaphore_wait(barrier, greeted)
    send(tok.at[c], tok.at[c], tsem, tp=1 - c)
    l_wor = load(wor_h, wor)
    l_woa = load(woa_h, woa)

    l_gain.wait()

    def scale_half(half):
        x = tok[half].astype(F32)
        scaled[half] = (x * gain[half]).astype(BF)
        return jnp.sum(x * x, axis=1, keepdims=True)

    squares = scale_half(c)
    for copy in l_own:
        copy.wait()
    acc[:, 0:256] = dot(scaled[c], wkv[own_rows, :])
    acc[:, 256:768] = dot(scaled[c], wr[own_rows, :])
    acc[:, 768:1280] = dot(scaled[c], wq[own_rows, :])

    arrived(tok.at[1 - c], tsem)
    squares = squares + scale_half(1 - c)
    inverse = lax.rsqrt(squares / D + EPS)
    for copy in l_kv:
        copy.wait()
    kv = (acc[:, 0:256] + dot(scaled[1 - c], wkv[other_rows, :])) * inverse
    kbuf[sp] = kv[:, 0:128].astype(BF)
    vbuf[sp] = jnp.transpose(kv[:, 128:256]).astype(BF)

    def slot(row, col):
        return row * YN + col

    def send_block(buf, sem, row, col, to, when):
        s = slot(row, col)
        send(buf.at[s], buf.at[s], sem.at[s], when=when, sp=to)

    goes_down = z <= BACK - 1

    def send_down(buf, sem, at, when):
        send(buf.at[at], buf.at[at], sem.at[at], when=when, sp=down)

    def forward_own(buf, sem, col):
        send_block(buf, sem, z, col, up, has_up)
        send_down(buf, sem, slot(z, col), goes_down)

    for step in (1, 3):
        send(kbuf.at[sp], kbuf.at[sp], ksem.at[sp], sp=beside(step))
    forward_own(vbuf, vsem, y)
    forward_own(kbuf, ksem, y)

    def plus(buf, sem, d, col):
        row = jnp.maximum(z - d, 0)
        ok = z >= d
        s = slot(row, col)
        arrived(buf.at[s], sem.at[s], ok)
        if d < FWD:
            send_block(buf, sem, row, col, up, ok & has_up)

    def minus(buf, sem, e, col):
        row = (z + e) % ZN
        ok = row <= BACK - 1
        s = slot(row, col)
        arrived(buf.at[s], sem.at[s], ok)
        if e < BACK:
            send_down(buf, sem, s, ok)

    def row_plus(d):
        return jnp.maximum(z - d, 0), z >= d

    def row_minus(e):
        row = (z + e) % ZN
        return row, (row <= BACK - 1) & (z > row)

    def spread_v(row, ok):
        way = 1 - 2 * (row % 2)
        send_block(vbuf, vsem, row, y, beside(way), ok)
        send_block(vbuf, vsem, row, y, beside(-way), ok)

    def relay_v(row, ok):
        way = 1 - 2 * (row % 2)
        s = slot(row, (y - way + YN) % YN)
        arrived(vbuf.at[s], vsem.at[s], ok)
        send(vbuf.at[s], vbuf.at[s], vsem.at[s], when=ok, sp=beside(way))

    def keys_beside():
        way = 2 * (z % 2) - 1
        for turn in (-way, way):
            col = (y + turn + YN) % YN
            s = slot(z, col)
            arrived(kbuf.at[s], ksem.at[s])
            if turn is not way:
                send(kbuf.at[s], kbuf.at[s], ksem.at[s], sp=beside(way))
            forward_own(kbuf, ksem, col)

    def keys_across():
        col = (y + 2) % YN
        s = slot(z, col)
        arrived(kbuf.at[s], ksem.at[s])
        forward_own(kbuf, ksem, col)

    def finish_v(row, ok):
        way = 1 - 2 * (row % 2)
        for col in ((y + way + YN) % YN, (y + 2) % YN):
            s = slot(row, col)
            arrived(vbuf.at[s], vsem.at[s], ok)

    always = z >= 0
    spread_v(z, always)

    l_r.wait()
    recur = ((acc[:, 256:768] + dot(scaled[1 - c], wr[other_rows, :])) * inverse).astype(BF)
    rin[...] = recur
    send(rin.at[pl.ds(ROWS - 16, 16)], halo, hsem, when=sp < SP - 1, sp=(sp + 1) % SP)
    xext[pl.ds(8, ROWS), :] = recur.astype(F32)


    def v_plus(d):
        plus(vbuf, vsem, d, y)
        spread_v(*row_plus(d))

    def v_minus(e):
        minus(vbuf, vsem, e, y)
        spread_v(*row_minus(e))

    l_q.wait()
    query = ((acc[:, 768:1280] + dot(scaled[1 - c], wq[other_rows, :])) * inverse).astype(BF)
    query = query.astype(F32) * HEAD ** (-0.5)
    qt[...] = jnp.zeros_like(qt)
    for h in range(4):
        turned = jnp.transpose(query[:, h * 128 : (h + 1) * 128]).astype(BF)
        lanes = slice((h % 2) * 128, (h % 2) * 128 + 128)
        qt[h // 2, 0:64, lanes] = turned[0:64]
        qt[2 + h // 2, 64:128, lanes] = turned[64:128]


    keys_beside()
    v_plus(1)
    v_minus(1)

    for copy in l_small:
        copy.wait()
    arrived(halo, hsem, sp > 0)
    before = halo[8:16, :].astype(F32)
    xext[pl.ds(0, 8), :] = jnp.where(sp > 0, before, 0.0)
    conv = jnp.zeros((ROWS, 512), F32)
    for k in range(4):
        conv = conv + cw[k : k + 1, :] * xext[pl.ds(5 + k, ROWS), :]
    conv = conv.astype(BF)
    gates[...] = jnp.zeros_like(gates)
    for j in range(4):
        for side in range(2):
            rows = slice(side * 64, side * 64 + 64)
            gates[j, rows, side * 64 : side * 64 + 64] = wgd[2 * j + side]
            gates[j, rows, 128 + side * 64 : 128 + side * 64 + 64] = wgi[2 * j + side]
    lane = lax.broadcasted_iota(jnp.int32, (ROWS, 128), 1)
    line = lax.broadcasted_iota(jnp.int32, (ROWS, 128), 0)
    extra_t = jnp.transpose(extra[...])
    def recur_columns(j):
        cols = slice(j * 128, j * 128 + 128)
        part = conv[:, cols]
        both = dot(part, gates[j])
        decay_gate = jax.nn.sigmoid(both[:, 0:128])
        input_gate = jax.nn.sigmoid(both[:, 128:256])
        added = jnp.where(lane < 64, extra_t[:, 2 * j : 2 * j + 1], extra_t[:, 2 * j + 1 : 2 * j + 2])
        log_decay = -RATE * decay_gate * base[:, cols] - added
        a = jnp.exp(log_decay)
        b = jnp.sqrt(minus_expm1(2.0 * log_decay)) * input_gate * part.astype(F32)
        for shift in (1, 2, 4, 8, 16, 32, 64):
            inside = line >= shift
            a_back = jnp.where(inside, pltpu.roll(a, shift, 0), 1.0)
            b_back = jnp.where(inside, pltpu.roll(b, shift, 0), 0.0)
            b = a * b_back + b
            a = a * a_back
        decs[:, cols] = a
        states[:, cols] = b
        crow[y, 0:1, cols] = a[ROWS - 1 : ROWS]
        crow[y, 1:2, cols] = b[ROWS - 1 : ROWS]


    recur_columns(0)
    recur_columns(1)
    plus(kbuf, ksem, 1, y)
    minus(kbuf, ksem, 1, y)
    relay_v(z, always)
    recur_columns(2)
    recur_columns(3)
    for step in (1, 3, 2):
        send(crow.at[y], crow.at[y], crsem.at[y], sp=beside(step))
    keys_across()
    v_plus(2)
    v_minus(2)
    relay_v(*row_plus(1))
    relay_v(*row_minus(1))

    def key(sign, n, step):
        move = plus if sign > 0 else minus
        return lambda: move(kbuf, ksem, n, (y + step) % YN)

    def attend(row, ok, parts, diagonal=False, steps=None):
        def run():
            if steps is None:
                first = row * YN
                keys = kbuf[pl.ds(first, YN)].reshape(YN * ROWS, 128)
                values = jnp.concatenate([vbuf[first + i] for i in range(YN)], axis=1)
            else:
                slots = [slot(row, (y + step) % YN) for step in steps]
                keys = jnp.concatenate([kbuf[s] for s in slots], axis=0)
                values = jnp.concatenate([vbuf[s] for s in slots], axis=1)
            all_scores = [dot(keys, qt[part]) for part in parts]
            for part, scores in zip(parts, all_scores):
                if diagonal:
                    key_at = lax.broadcasted_iota(jnp.int32, scores.shape, 0)
                    query_at = lax.broadcasted_iota(jnp.int32, scores.shape, 1) % ROWS + y * ROWS
                    scores = jnp.where(query_at >= key_at, scores, -1e30)
                    new = jnp.max(scores, axis=0, keepdims=True)
                    weights = jnp.exp(scores - new)
                    total[part] = jnp.sum(weights, axis=0, keepdims=True)
                    att[part] = dot(values, weights.astype(BF))
                else:
                    old = peak[part]
                    new = jnp.maximum(old, jnp.max(scores, axis=0, keepdims=True))
                    weights = jnp.exp(scores - new)
                    fade = jnp.exp(old - new)
                    total[part] = total[part] * fade + jnp.sum(weights, axis=0, keepdims=True)
                    att[part] = att[part] * fade + dot(values, weights.astype(BF))
                peak[part] = new

        if ok is None:
            run()
        else:
            pl.when(ok)(run)

    fillers = []

    def filler():
        if fillers:
            fillers.pop(0)()

    def ready(row, ok, **how):
        for parts in ((0, 1, 2, 3),) if "steps" in how else ((0, 1), (2, 3)):
            fillers.append(lambda parts=parts: attend(row, ok, parts, **how))

    def run(*ops):
        for op in ops:
            op()
            filler()

    def row_carry():
        for step in (1, 3, 2):
            col = (y + step) % YN
            arrived(crow.at[col], crsem.at[col])
        all_a = crow[0, 0:1, :]
        all_s = crow[0, 1:2, :]
        for col in range(1, YN):
            all_s = crow[col, 0:1, :] * all_s + crow[col, 1:2, :]
            all_a = crow[col, 0:1, :] * all_a
        ctot[z, 0:1, :] = all_a
        ctot[z, 1:2, :] = all_s
        send(ctot.at[z], ctot.at[z], ctsem.at[z], when=has_up, sp=up)
        send_down(ctot, ctsem, z, goes_down)

    def carry(n):
        row, ok = row_plus(n)
        arrived(ctot.at[row], ctsem.at[row], ok)
        if n < FWD:
            send(ctot.at[row], ctot.at[row], ctsem.at[row], when=ok & has_up, sp=up)
        if n <= BACK:
            row = (z + n) % ZN
            ok = row <= BACK - 1
            arrived(ctot.at[row], ctsem.at[row], ok)
            if n < BACK:
                send_down(ctot, ctsem, row, ok)

    def fold_total(row, s):
        return ctot[row, 0:1, :] * s + ctot[row, 1:2, :]

    def fold_row(col, s):
        return crow[col, 0:1, :] * s + crow[col, 1:2, :]

    def recur_output():
        carry_in = lax.fori_loop(0, z, fold_total, jnp.zeros((1, 512), F32))
        carry_in = lax.fori_loop(0, y, fold_row, carry_in)
        rout[...] = (states[...] + decs[...] * carry_in).astype(BF)
        l_wor.wait()

    def recur_project(n):
        mbuf[n] = dot(rout[...], wor[:, n * 512 : n * 512 + 512])

    def drain():
        while sends:
            copy, when = sends.pop(0)
            if when is None:
                copy.wait_send()
            else:
                pl.when(when)(lambda copy=copy: copy.wait_send())

    finish_v(z, always)
    ready(z, None, diagonal=True)
    run(key(1, 1, 1), key(-1, 1, 1), key(1, 1, 3), key(-1, 1, 3))
    run(key(1, 2, 0), key(-1, 2, 0), key(1, 1, 2), key(-1, 1, 2))
    run(lambda: v_plus(3), lambda: v_minus(3))
    run(lambda: relay_v(*row_plus(2)), lambda: relay_v(*row_minus(2)), lambda: finish_v(*row_plus(1)))
    ready(*row_plus(1))
    run(lambda: finish_v(*row_minus(1)))
    ready(*row_minus(1))
    run(row_carry, key(1, 2, 1), key(-1, 2, 1), key(1, 2, 3), key(-1, 2, 3))
    run(key(1, 3, 0), key(-1, 3, 0), key(1, 2, 2), key(-1, 2, 2))
    run(lambda: v_plus(4), lambda: relay_v(*row_plus(3)), lambda: relay_v(*row_minus(3)))
    run(lambda: finish_v(*row_plus(2)))
    ready(*row_plus(2))
    run(lambda: carry(1), lambda: finish_v(*row_minus(2)))
    ready(*row_minus(2))
    run(key(1, 3, 1), key(-1, 3, 1), lambda: carry(2), key(1, 3, 3), key(-1, 3, 3))
    run(key(1, 4, 0), key(1, 3, 2), key(-1, 3, 2))
    run(lambda: relay_v(*row_plus(4)), lambda: finish_v(*row_plus(3)))
    ready(*row_plus(3))
    run(lambda: carry(3), lambda: finish_v(*row_minus(3)))
    ready(*row_minus(3))
    run(key(1, 4, 1), lambda: carry(4), key(1, 4, 3), drain, lambda: finish_v(*row_plus(4)))
    fillers.append(recur_output)
    for n in range(4):
        fillers.append(lambda n=n: recur_project(n))
    while fillers:
        filler()
    key(1, 4, 2)()
    attend(*row_plus(4), (0, 1), steps=(0, 1, 3, 2))
    attend(*row_plus(4), (2, 3), steps=(0, 1, 3, 2))

    pieces = []
    for h in range(4):
        lanes = slice((h % 2) * 128, (h % 2) * 128 + 128)
        first = att[h // 2, :, lanes] / total[h // 2, :, lanes]
        second = att[2 + h // 2, :, lanes] / total[2 + h // 2, :, lanes]
        out = first - lam[0:1, h : h + 1] * second
        out = out * lax.rsqrt(jnp.mean(out * out, axis=0, keepdims=True) + EPS)
        pieces.append((jnp.transpose(out) * hgain[...]).astype(BF))
    attend_out = jnp.concatenate(pieces, axis=1)

    mine = pl.ds(pl.multiple_of(c * 64, 64), 64)
    theirs = pl.ds(pl.multiple_of((1 - c) * 64, 64), 64)
    l_woa.wait()
    for n in range(4):
        mbuf[n] += dot(attend_out, woa[:, n * 512 : n * 512 + 512])
        send(mbuf.at[n, theirs], mrecv.at[n], msem.at[n], tp=1 - c)
    power = jnp.zeros((64, 1), F32)
    for n in range(4):
        arrived(mrecv.at[n], msem.at[n])
        whole = mbuf[n, mine, :] + mrecv[n]
        mrecv[n] = whole
        power = power + jnp.sum(whole * whole, axis=1, keepdims=True)
    scale = lax.rsqrt(power / D + EPS)
    for n in range(4):
        cols = slice(n * 512, n * 512 + 512)
        out_h[:, cols] = (mrecv[n] * scale * ogain[:, cols]).astype(BF)
    drain()


def body(
    tokens, norm_gain, w_recur_in, conv_weight, w_gate_decay, w_gate_input, decay_base, extra_decay,
    w_query, w_key, w_value, mix_lambda, head_gain, w_out_recur, w_out_attend, out_gain,
):
    any_ = pl.BlockSpec(memory_space=pl.ANY)
    vmem = pltpu.VMEM
    dma = pltpu.SemaphoreType.DMA
    scratch = [
        vmem((2, ROWS, HALF), BF), vmem((2, 1, HALF), F32), vmem((D, 512), BF), vmem((4, 512), F32),
        vmem((8, 64, 64), BF), vmem((8, 64, 64), BF), vmem((1, 512), F32), vmem((8, ROWS), F32),
        vmem((D, 512), BF), vmem((D, 256), BF), vmem((1, 4), F32), vmem((1, 128), F32),
        vmem((512, D), BF), vmem((512, D), BF), vmem((1, D), F32),
        vmem((2, ROWS, HALF), BF), vmem((ROWS, 1280), F32),
        vmem((SP, ROWS, 128), BF), vmem((SP, 128, ROWS), BF),
        vmem((ROWS, 512), BF), vmem((16, 512), BF), vmem((ROWS + 8, 512), F32),
        vmem((4, 128, 256), BF), vmem((4, 128, 256), F32), vmem((4, 1, 256), F32), vmem((4, 1, 256), F32),
        vmem((4, 128, 256), BF),
        vmem((YN, 2, 512), F32), vmem((ZN, 2, 512), F32), vmem((ROWS, 512), F32), vmem((ROWS, 512), F32),
        vmem((4, ROWS, 512), F32), vmem((4, 64, 512), F32), vmem((ROWS, 512), BF),
        dma((24,)), dma((NSEND,)), dma, dma((SP,)), dma((SP,)), dma, dma((YN,)), dma((ZN,)), dma((4,)),
    ]
    return pl.pallas_call(
        kernel,
        out_shape=pltpu.VMEM((64, D), BF),
        in_specs=[any_] * 16,
        out_specs=pl.BlockSpec(memory_space=pltpu.VMEM),
        scratch_shapes=scratch,
        compiler_params=pltpu.CompilerParams(
            collective_id=0, has_side_effects=True, vmem_limit_bytes=60 * 1024 * 1024
        ),
        name="layer",
    )(
        tokens, norm_gain.reshape(2, 1, HALF), w_recur_in, conv_weight, w_gate_decay, w_gate_input,
        decay_base.reshape(1, -1), extra_decay.T, w_query, w_key, w_value, mix_lambda.reshape(1, -1),
        head_gain.reshape(1, -1), w_out_recur, w_out_attend, out_gain.reshape(1, -1),
    )


def solution(mesh):
    in_specs = (
        P(("fs", "sp"), "tp"),
        P(),
        P(None, "tp"),
        P(None, "tp"),
        P("tp", None, None),
        P("tp", None, None),
        P("tp"),
        P(("fs", "sp"), "tp"),
        P(None, "tp"),
        P(None, "tp"),
        P(None, "tp"),
        P("tp"),
        P(),
        P("tp", None),
        P("tp", None),
        P(),
    )
    out_specs = P(("fs", "sp", "tp"), None)
    return jax.shard_map(body, mesh=mesh, in_specs=in_specs, out_specs=out_specs, check_vma=False)
```

```python
import jax
import jax.numpy as jnp
from jax import lax
from jax.experimental import pallas as pl
from jax.experimental.pallas import tpu as pltpu
from jax.sharding import PartitionSpec as P

MESH = pl.DeviceIdType.MESH
BF = jnp.bfloat16
F32 = jnp.float32

D = 2048
HALF = 1024
HEAD = 64
ROWS = 128
ZN = 8
YN = 4
SP = ZN * YN
RATE = 8.0
EPS = 1e-06
FWD = 3
BACK = 4
NSEND = 144


def dot(a, b):
    return jnp.dot(a, b, preferred_element_type=F32)


def minus_expm1(x):
    series = 1.0 + x * (
        1 / 2 + x * (1 / 6 + x * (1 / 24 + x * (1 / 120 + x * (1 / 720 + x * (1 / 5040 + x / 40320)))))
    )
    return jnp.where(x > -0.5, -x * series, 1.0 - jnp.exp(x))


def kernel(
    tok_h, gain_h, wr_h, cw_h, wgd_h, wgi_h, base_h, extra_h, wq_h, wk_h, wv_h, lam_h, hgain_h,
    wor_h, woa_h, ogain_h, out_h,
    tok, gain, wr, cw, wgd, wgi, base, extra, wq, wkv, lam, hgain, wor, woa, ogain,
    scaled, acc, kbuf, vbuf, rin, halo, xext, qt, att, peak, total, gates,
    crow, ctot, decs, states, mbuf, mrecv, rout,
    lsem, ssem, tsem, ksem, vsem, hsem, crsem, ctsem, msem, known,
):
    sp = lax.axis_index("sp")
    c = lax.axis_index("tp")
    z = sp // YN
    y = sp % YN

    locals_ = []

    def load(src, dst):
        copy = pltpu.make_async_copy(src, dst, lsem.at[len(locals_)])
        locals_.append(copy)
        copy.start()
        return copy

    own_rows = pl.ds(pl.multiple_of(c * HALF, HALF), HALF)
    other_rows = pl.ds(pl.multiple_of((1 - c) * HALF, HALF), HALF)
    l_tok = load(tok_h, tok.at[c])
    l_gain = load(gain_h, gain)
    l_own = [
        load(wk_h.at[own_rows], wkv.at[own_rows, pl.ds(0, 128)]),
        load(wv_h.at[own_rows], wkv.at[own_rows, pl.ds(128, 128)]),
        load(wr_h.at[own_rows], wr.at[own_rows]),
        load(wq_h.at[own_rows], wq.at[own_rows]),
    ]
    l_kv = [
        load(wk_h.at[other_rows], wkv.at[other_rows, pl.ds(0, 128)]),
        load(wv_h.at[other_rows], wkv.at[other_rows, pl.ds(128, 128)]),
    ]
    l_r = load(wr_h.at[other_rows], wr.at[other_rows])
    l_q = load(wq_h.at[other_rows], wq.at[other_rows])
    l_small = [
        load(cw_h, cw), load(wgd_h, wgd), load(wgi_h, wgi), load(base_h, base), load(extra_h, extra),
        load(lam_h, lam), load(hgain_h, hgain), load(ogain_h, ogain),
    ]

    barrier = pltpu.get_barrier_semaphore()
    pl.semaphore_signal(barrier, inc=1, device_id={"tp": 1 - c}, device_id_type=MESH)
    for step in (1, 2, 3):
        pl.semaphore_signal(
            barrier, inc=1, device_id={"sp": z * YN + (y + step) % YN}, device_id_type=MESH
        )
    has_up = z < ZN - 1
    has_down = z > 0
    around = (z == 0) | (z == ZN - 1)
    corner_up = (y == YN - 1) & has_up
    corner_down = (y == 0) & has_down
    greeted = 4
    for when, target in (
        (has_up, (z + 1) * YN + y), (has_down, (z - 1) * YN + y), (around, (ZN - 1 - z) * YN + y),
        (corner_up, sp + 1), (corner_down, sp - 1),
    ):
        near = jnp.where(when, target, sp)

        @pl.when(when)
        def _():
            pl.semaphore_signal(barrier, inc=1, device_id={"sp": near}, device_id_type=MESH)

        greeted = greeted + when.astype(jnp.int32)

    sends = []
    numbers = iter(range(NSEND))

    def send(src, dst, rsem, when=None, **target):
        copy = pltpu.make_async_remote_copy(
            src_ref=src, dst_ref=dst, send_sem=ssem.at[next(numbers)], recv_sem=rsem,
            device_id=target, device_id_type=MESH,
        )
        sends.append((copy, when))
        if when is None:
            copy.start()
        else:
            pl.when(when)(lambda: copy.start())

    def arrived(dst, rsem, when=None):
        copy = pltpu.make_async_remote_copy(
            src_ref=dst, dst_ref=dst, send_sem=ssem.at[0], recv_sem=rsem,
            device_id={"tp": 1 - c}, device_id_type=MESH,
        )
        if when is None:
            copy.wait_recv()
        else:
            pl.when(when)(lambda: copy.wait_recv())

    up = ((z + 1) % ZN) * YN + y
    down = ((z + ZN - 1) % ZN) * YN + y

    def beside(step):
        return z * YN + (y + step + YN) % YN

    def tell(n, distance):
        pl.semaphore_signal(
            known.at[n], inc=1, device_id={"sp": ((z + distance) % ZN) * YN + y}, device_id_type=MESH
        )

    l_tok.wait()
    pl.semaphore_wait(barrier, greeted)
    send(tok.at[c], tok.at[c], tsem, tp=1 - c)
    l_wor = load(wor_h, wor)
    l_woa = load(woa_h, woa)

    l_gain.wait()

    def scale_half(half):
        x = tok[half].astype(F32)
        scaled[half] = (x * gain[half]).astype(BF)
        return jnp.sum(x * x, axis=1, keepdims=True)

    squares = scale_half(c)
    tell(0, 1)
    tell(1, ZN - 1)
    for copy in l_own:
        copy.wait()
    acc[:, 0:256] = dot(scaled[c], wkv[own_rows, :])
    acc[:, 256:768] = dot(scaled[c], wr[own_rows, :])
    acc[:, 768:1280] = dot(scaled[c], wq[own_rows, :])

    arrived(tok.at[1 - c], tsem)
    squares = squares + scale_half(1 - c)
    inverse = lax.rsqrt(squares / D + EPS)
    for copy in l_kv:
        copy.wait()
    kv = (acc[:, 0:256] + dot(scaled[1 - c], wkv[other_rows, :])) * inverse
    kbuf[sp] = kv[:, 0:128].astype(BF)
    vbuf[sp] = jnp.transpose(kv[:, 128:256]).astype(BF)

    def slot(row, col):
        return row * YN + col

    def send_block(buf, sem, row, col, to, when):
        s = slot(row, col)
        send(buf.at[s], buf.at[s], sem.at[s], when=when, sp=to)

    goes_down = z <= BACK - 1

    def send_down(buf, sem, at, when):
        send(buf.at[at], buf.at[at], sem.at[at], when=when, sp=down)

    def forward_own(buf, sem, col):
        send_block(buf, sem, z, col, up, has_up)
        send_down(buf, sem, slot(z, col), goes_down)

    for step in (1, 3, 2):
        send(kbuf.at[sp], kbuf.at[sp], ksem.at[sp], sp=beside(step))
    forward_own(vbuf, vsem, y)
    forward_own(kbuf, ksem, y)

    def plus(buf, sem, d, col):
        row = jnp.maximum(z - d, 0)
        ok = z >= d
        s = slot(row, col)
        arrived(buf.at[s], sem.at[s], ok)
        if d < FWD:
            send_block(buf, sem, row, col, up, ok & has_up)

    def minus(buf, sem, e, col):
        row = (z + e) % ZN
        ok = row <= BACK - 1
        s = slot(row, col)
        arrived(buf.at[s], sem.at[s], ok)
        if e < BACK:
            send_down(buf, sem, s, ok)

    def row_plus(d):
        return jnp.maximum(z - d, 0), z >= d

    def row_minus(e):
        row = (z + e) % ZN
        return row, (row <= BACK - 1) & (z > row)

    def spread_v(row, ok, across=False):
        way = 1 - 2 * (row % 2)
        send_block(vbuf, vsem, row, y, beside(way), ok)
        send_block(vbuf, vsem, row, y, beside(-way), ok)
        if across:
            send_block(vbuf, vsem, row, y, beside(2), ok)

    def relay_v(row, ok):
        way = 1 - 2 * (row % 2)
        s = slot(row, (y - way + YN) % YN)
        arrived(vbuf.at[s], vsem.at[s], ok)
        send(vbuf.at[s], vbuf.at[s], vsem.at[s], when=ok, sp=beside(way))

    def keys_beside():
        for step in (1, 3):
            col = (y + step) % YN
            s = slot(z, col)
            arrived(kbuf.at[s], ksem.at[s])
            forward_own(kbuf, ksem, col)

    def keys_across():
        col = (y + 2) % YN
        s = slot(z, col)
        arrived(kbuf.at[s], ksem.at[s])
        forward_own(kbuf, ksem, col)

    def finish_v(row, ok, across=False):
        way = 1 - 2 * (row % 2)
        cols = [(y + way + YN) % YN, (y + 2) % YN]
        if across:
            cols.append((y - way + YN) % YN)
        for col in cols:
            s = slot(row, col)
            arrived(vbuf.at[s], vsem.at[s], ok)

    always = z >= 0
    spread_v(z, always)

    l_r.wait()
    recur = ((acc[:, 256:768] + dot(scaled[1 - c], wr[other_rows, :])) * inverse).astype(BF)
    rin[...] = recur
    send(rin.at[pl.ds(ROWS - 16, 16)], halo, hsem, when=sp < SP - 1, sp=(sp + 1) % SP)
    xext[pl.ds(8, ROWS), :] = recur.astype(F32)


    def v_plus(d):
        plus(vbuf, vsem, d, y)
        spread_v(*row_plus(d), across=d == FWD)

    def v_minus(e):
        minus(vbuf, vsem, e, y)
        spread_v(*row_minus(e), across=e == BACK)

    l_q.wait()
    query = ((acc[:, 768:1280] + dot(scaled[1 - c], wq[other_rows, :])) * inverse).astype(BF)
    query = query.astype(F32) * HEAD ** (-0.5)
    qt[...] = jnp.zeros_like(qt)
    for h in range(4):
        turned = jnp.transpose(query[:, h * 128 : (h + 1) * 128]).astype(BF)
        lanes = slice((h % 2) * 128, (h % 2) * 128 + 128)
        qt[h // 2, 0:64, lanes] = turned[0:64]
        qt[2 + h // 2, 64:128, lanes] = turned[64:128]


    def attend(row, ok, steps=(), first_of_all=False, earlier=False):
        def run():
            if steps:
                slots = [slot(row, (y + step) % YN) for step in steps]
                keys = jnp.concatenate([kbuf[s] for s in slots], axis=0)
                values = jnp.concatenate([vbuf[s] for s in slots], axis=1)
            else:
                first = row * YN
                keys = kbuf[pl.ds(first, YN)].reshape(YN * ROWS, 128)
                values = jnp.concatenate([vbuf[first + i] for i in range(YN)], axis=1)
            all_scores = [dot(keys, qt[part]) for part in range(4)]
            for part, scores in enumerate(all_scores):
                if first_of_all:
                    key_at = lax.broadcasted_iota(jnp.int32, scores.shape, 0)
                    query_at = lax.broadcasted_iota(jnp.int32, scores.shape, 1) % ROWS
                    scores = jnp.where(query_at >= key_at, scores, -1e30)
                    new = jnp.max(scores, axis=0, keepdims=True)
                    weights = jnp.exp(scores - new)
                    total[part] = jnp.sum(weights, axis=0, keepdims=True)
                    att[part] = dot(values, weights.astype(BF))
                else:
                    if earlier:
                        scores = jnp.concatenate(
                            [
                                jnp.where((y + step) % YN < y, scores[n * ROWS : n * ROWS + ROWS], -1e30)
                                for n, step in enumerate(steps)
                            ],
                            axis=0,
                        )
                    old = peak[part]
                    new = jnp.maximum(old, jnp.max(scores, axis=0, keepdims=True))
                    weights = jnp.exp(scores - new)
                    fade = jnp.exp(old - new)
                    total[part] = total[part] * fade + jnp.sum(weights, axis=0, keepdims=True)
                    att[part] = att[part] * fade + dot(values, weights.astype(BF))
                peak[part] = new

        if ok is None:
            run()
        else:
            pl.when(ok)(run)

    attend(z, None, steps=(0,), first_of_all=True)
    v_plus(1)
    v_minus(1)
    keys_beside()
    plus(kbuf, ksem, 1, y)
    minus(kbuf, ksem, 1, y)
    relay_v(z, always)
    pl.semaphore_wait(known.at[0], 1)
    pl.semaphore_wait(known.at[1], 1)
    tell(2, 2)
    tell(3, ZN - 2)

    for copy in l_small:
        copy.wait()
    arrived(halo, hsem, sp > 0)
    before = halo[8:16, :].astype(F32)
    xext[pl.ds(0, 8), :] = jnp.where(sp > 0, before, 0.0)
    conv = jnp.zeros((ROWS, 512), F32)
    for k in range(4):
        conv = conv + cw[k : k + 1, :] * xext[pl.ds(5 + k, ROWS), :]
    conv = conv.astype(BF)
    gates[...] = jnp.zeros_like(gates)
    for j in range(4):
        for side in range(2):
            rows = slice(side * 64, side * 64 + 64)
            gates[j, rows, side * 64 : side * 64 + 64] = wgd[2 * j + side]
            gates[j, rows, 128 + side * 64 : 128 + side * 64 + 64] = wgi[2 * j + side]
    lane = lax.broadcasted_iota(jnp.int32, (ROWS, 128), 1)
    line = lax.broadcasted_iota(jnp.int32, (ROWS, 128), 0)
    extra_t = jnp.transpose(extra[...])
    def recur_columns(j):
        cols = slice(j * 128, j * 128 + 128)
        part = conv[:, cols]
        both = dot(part, gates[j])
        decay_gate = jax.nn.sigmoid(both[:, 0:128])
        input_gate = jax.nn.sigmoid(both[:, 128:256])
        added = jnp.where(lane < 64, extra_t[:, 2 * j : 2 * j + 1], extra_t[:, 2 * j + 1 : 2 * j + 2])
        log_decay = -RATE * decay_gate * base[:, cols] - added
        a = jnp.exp(log_decay)
        b = jnp.sqrt(minus_expm1(2.0 * log_decay)) * input_gate * part.astype(F32)
        for shift in (1, 2, 4, 8, 16, 32, 64):
            inside = line >= shift
            a_back = jnp.where(inside, pltpu.roll(a, shift, 0), 1.0)
            b_back = jnp.where(inside, pltpu.roll(b, shift, 0), 0.0)
            b = a * b_back + b
            a = a * a_back
        decs[:, cols] = a
        states[:, cols] = b
        crow[y, 0:1, cols] = a[ROWS - 1 : ROWS]
        crow[y, 1:2, cols] = b[ROWS - 1 : ROWS]


    recur_columns(0)
    recur_columns(1)
    keys_across()
    v_plus(2)
    v_minus(2)
    recur_columns(2)
    recur_columns(3)
    for step in (1, 3, 2):
        send(crow.at[y], crow.at[y], crsem.at[y], sp=beside(step))
    relay_v(*row_plus(1))
    relay_v(*row_minus(1))

    def key(sign, n, step):
        move = plus if sign > 0 else minus
        return lambda: move(kbuf, ksem, n, (y + step) % YN)

    def row_carry():
        for step in (1, 3, 2):
            col = (y + step) % YN
            arrived(crow.at[col], crsem.at[col])
        all_a = crow[0, 0:1, :]
        all_s = crow[0, 1:2, :]
        for col in range(1, YN):
            all_s = crow[col, 0:1, :] * all_s + crow[col, 1:2, :]
            all_a = crow[col, 0:1, :] * all_a
        ctot[z, 0:1, :] = all_a
        ctot[z, 1:2, :] = all_s
        pl.semaphore_wait(known.at[2], 1)
        pl.semaphore_wait(known.at[3], 1)
        for distance in range(1, ZN):
            to = ((z + distance) % ZN) * YN + y
            send(ctot.at[z], ctot.at[z], ctsem.at[z], when=z + distance < ZN, sp=to)

    def carries():
        for row in range(ZN - 1):
            arrived(ctot.at[row], ctsem.at[row], row < z)

    def fold_total(row, s):
        return ctot[row, 0:1, :] * s + ctot[row, 1:2, :]

    def fold_row(col, s):
        return crow[col, 0:1, :] * s + crow[col, 1:2, :]

    def recur_output():
        carry_in = lax.fori_loop(0, z, fold_total, jnp.zeros((1, 512), F32))
        carry_in = lax.fori_loop(0, y, fold_row, carry_in)
        rout[...] = (states[...] + decs[...] * carry_in).astype(BF)
        l_wor.wait()

    def recur_project(n):
        mbuf[n] = dot(rout[...], wor[:, n * 512 : n * 512 + 512])

    def drain():
        while sends:
            copy, when = sends.pop(0)
            if when is None:
                copy.wait_send()
            else:
                pl.when(when)(lambda copy=copy: copy.wait_send())

    def both(n, *steps):
        for step in steps:
            if n <= FWD:
                key(1, n, step)()
            if n <= BACK:
                key(-1, n, step)()

    both(1, 1, 3)
    finish_v(z, always)
    attend(z, None, steps=(1, 2, 3), earlier=True)
    both(2, 0)
    v_plus(3)
    v_minus(3)
    both(1, 2)
    finish_v(*row_plus(1))
    finish_v(*row_minus(1))
    relay_v(*row_plus(2))
    relay_v(*row_minus(2))
    row_carry()
    attend(*row_plus(1))
    both(2, 1, 3)
    both(3, 0)
    v_minus(4)
    attend(*row_minus(1))
    relay_v(*row_minus(3))
    both(2, 2)
    finish_v(*row_plus(2))
    finish_v(*row_minus(2))
    attend(*row_plus(2))
    both(3, 1, 3)
    both(4, 0)
    attend(*row_minus(2))
    both(3, 2)
    finish_v(*row_plus(3), across=True)
    finish_v(*row_minus(3))
    attend(*row_plus(3))
    both(4, 1, 3)
    attend(*row_minus(3))
    drain()
    carries()
    recur_output()
    for n in range(4):
        recur_project(n)
    finish_v(*row_minus(4), across=True)
    both(4, 2)
    attend(*row_minus(4))

    pieces = []
    for h in range(4):
        lanes = slice((h % 2) * 128, (h % 2) * 128 + 128)
        first = att[h // 2, :, lanes] / total[h // 2, :, lanes]
        second = att[2 + h // 2, :, lanes] / total[2 + h // 2, :, lanes]
        out = first - lam[0:1, h : h + 1] * second
        out = out * lax.rsqrt(jnp.mean(out * out, axis=0, keepdims=True) + EPS)
        pieces.append((jnp.transpose(out) * hgain[...]).astype(BF))
    attend_out = jnp.concatenate(pieces, axis=1)

    mine = pl.ds(pl.multiple_of(c * 64, 64), 64)
    theirs = pl.ds(pl.multiple_of((1 - c) * 64, 64), 64)
    l_woa.wait()
    for n in range(4):
        mbuf[n] += dot(attend_out, woa[:, n * 512 : n * 512 + 512])
        send(mbuf.at[n, theirs], mrecv.at[n], msem.at[n], tp=1 - c)
    power = jnp.zeros((64, 1), F32)
    for n in range(4):
        arrived(mrecv.at[n], msem.at[n])
        whole = mbuf[n, mine, :] + mrecv[n]
        mrecv[n] = whole
        power = power + jnp.sum(whole * whole, axis=1, keepdims=True)
    scale = lax.rsqrt(power / D + EPS)
    for n in range(4):
        cols = slice(n * 512, n * 512 + 512)
        out_h[:, cols] = (mrecv[n] * scale * ogain[:, cols]).astype(BF)
    drain()


def body(
    tokens, norm_gain, w_recur_in, conv_weight, w_gate_decay, w_gate_input, decay_base, extra_decay,
    w_query, w_key, w_value, mix_lambda, head_gain, w_out_recur, w_out_attend, out_gain,
):
    any_ = pl.BlockSpec(memory_space=pl.ANY)
    vmem = pltpu.VMEM
    dma = pltpu.SemaphoreType.DMA
    scratch = [
        vmem((2, ROWS, HALF), BF), vmem((2, 1, HALF), F32), vmem((D, 512), BF), vmem((4, 512), F32),
        vmem((8, 64, 64), BF), vmem((8, 64, 64), BF), vmem((1, 512), F32), vmem((8, ROWS), F32),
        vmem((D, 512), BF), vmem((D, 256), BF), vmem((1, 4), F32), vmem((1, 128), F32),
        vmem((512, D), BF), vmem((512, D), BF), vmem((1, D), F32),
        vmem((2, ROWS, HALF), BF), vmem((ROWS, 1280), F32),
        vmem((SP, ROWS, 128), BF), vmem((SP, 128, ROWS), BF),
        vmem((ROWS, 512), BF), vmem((16, 512), BF), vmem((ROWS + 8, 512), F32),
        vmem((4, 128, 256), BF), vmem((4, 128, 256), F32), vmem((4, 1, 256), F32), vmem((4, 1, 256), F32),
        vmem((4, 128, 256), BF),
        vmem((YN, 2, 512), F32), vmem((ZN, 2, 512), F32), vmem((ROWS, 512), F32), vmem((ROWS, 512), F32),
        vmem((4, ROWS, 512), F32), vmem((4, 64, 512), F32), vmem((ROWS, 512), BF),
        dma((24,)), dma((NSEND,)), dma, dma((SP,)), dma((SP,)), dma, dma((YN,)), dma((ZN,)), dma((4,)),
        pltpu.SemaphoreType.REGULAR((4,)),
    ]
    return pl.pallas_call(
        kernel,
        out_shape=pltpu.VMEM((64, D), BF),
        in_specs=[any_] * 16,
        out_specs=pl.BlockSpec(memory_space=pltpu.VMEM),
        scratch_shapes=scratch,
        compiler_params=pltpu.CompilerParams(
            collective_id=0, has_side_effects=True, vmem_limit_bytes=60 * 1024 * 1024
        ),
        name="layer",
    )(
        tokens, norm_gain.reshape(2, 1, HALF), w_recur_in, conv_weight, w_gate_decay, w_gate_input,
        decay_base.reshape(1, -1), extra_decay.T, w_query, w_key, w_value, mix_lambda.reshape(1, -1),
        head_gain.reshape(1, -1), w_out_recur, w_out_attend, out_gain.reshape(1, -1),
    )


def solution(mesh):
    in_specs = (
        P(("fs", "sp"), "tp"),
        P(),
        P(None, "tp"),
        P(None, "tp"),
        P("tp", None, None),
        P("tp", None, None),
        P("tp"),
        P(("fs", "sp"), "tp"),
        P(None, "tp"),
        P(None, "tp"),
        P(None, "tp"),
        P("tp"),
        P(),
        P("tp", None),
        P("tp", None),
        P(),
    )
    out_specs = P(("fs", "sp", "tp"), None)
    return jax.shard_map(body, mesh=mesh, in_specs=in_specs, out_specs=out_specs, check_vma=False)
```

```python
import itertools

import jax
import jax.numpy as jnp
from jax import lax
from jax.experimental import pallas as pl
from jax.experimental.pallas import tpu as pltpu
from jax.sharding import PartitionSpec as P

MESH = pl.DeviceIdType.MESH
BF = jnp.bfloat16
F32 = jnp.float32

D = 2048
HALF = 1024
HEAD = 64
ROWS = 128
ZN = 8
YN = 4
SP = ZN * YN
RATE = 8.0
EPS = 1e-06
FWD = 4
BACK = 3
NSEND = 28


def dot(a, b):
    return jnp.dot(a, b, preferred_element_type=F32)


def minus_expm1(x):
    series = 1.0 + x * (
        1 / 2 + x * (1 / 6 + x * (1 / 24 + x * (1 / 120 + x * (1 / 720 + x * (1 / 5040 + x / 40320)))))
    )
    return jnp.where(x > -0.5, -x * series, 1.0 - jnp.exp(x))


def kernel(
    tok_h, gain_h, wr_h, cw_h, wgd_h, wgi_h, base_h, extra_h, wq_h, wk_h, wv_h, lam_h, hgain_h,
    wor_h, woa_h, ogain_h, out_h,
    tok, gain, wall, cw, wgd, wgi, base, extra, lam, hgain, wor, woa, ogain,
    scaled, acc, kbuf, vbuf, rin, halo, xext, qt, att, peak, total, gates,
    crow, ctot, decs, states, mbuf, mrecv, mpart, rout,
    lsem, ssem, tsem, ksem, vsem, hsem, crsem, ctsem, msem, known,
):
    sp = lax.axis_index("sp")
    c = lax.axis_index("tp")
    z = sp // YN
    y = sp % YN

    def load(n, *pairs):
        for src, dst in pairs:
            pltpu.make_async_copy(src, dst, lsem.at[n]).start()

    def loaded(n, dst):
        pltpu.make_async_copy(dst, dst, lsem.at[n]).wait()

    own_rows = pl.ds(pl.multiple_of(c * HALF, HALF), HALF)
    other_rows = pl.ds(pl.multiple_of((1 - c) * HALF, HALF), HALF)
    kv_cols, r_cols, q_cols = pl.ds(0, 256), pl.ds(256, 512), pl.ds(768, 512)
    load(0, (tok_h, tok.at[c]))
    load(1, (gain_h, gain))

    def load_kv(n, rows):
        load(n, (wk_h.at[rows], wall.at[rows, pl.ds(0, 128)]), (wv_h.at[rows], wall.at[rows, pl.ds(128, 128)]))

    load_kv(2, own_rows)
    load(2, (wr_h.at[own_rows], wall.at[own_rows, r_cols]), (wq_h.at[own_rows], wall.at[own_rows, q_cols]))
    load_kv(3, other_rows)
    load(4, (wr_h.at[other_rows], wall.at[other_rows, r_cols]))
    load(5, (wq_h.at[other_rows], wall.at[other_rows, q_cols]))

    barrier = pltpu.get_barrier_semaphore()
    pl.semaphore_signal(barrier, inc=1, device_id={"tp": 1 - c}, device_id_type=MESH)
    for step in (1, 2, 3):
        pl.semaphore_signal(
            barrier, inc=1, device_id={"sp": z * YN + (y + step) % YN}, device_id_type=MESH
        )
    has_up = z < ZN - 1
    has_down = z > 0
    around = (z == 0) | (z == ZN - 1)
    corner_up = (y == YN - 1) & has_up
    corner_down = (y == 0) & has_down
    greeted = 4
    for when, target in (
        (has_up, (z + 1) * YN + y), (has_down, (z - 1) * YN + y), (around, (ZN - 1 - z) * YN + y),
        (corner_up, sp + 1), (corner_down, sp - 1),
    ):
        near = jnp.where(when, target, sp)

        @pl.when(when)
        def _():
            pl.semaphore_signal(barrier, inc=1, device_id={"sp": near}, device_id_type=MESH)

        greeted = greeted + when.astype(jnp.int32)

    sends = []
    numbers = itertools.count()

    def settle(copy, when):
        if when is None:
            copy.wait_send()
        else:
            pl.when(when)(lambda: copy.wait_send())

    def send(src, dst, rsem, when=None, **target):
        if len(sends) == NSEND:
            settle(*sends.pop(0))
        copy = pltpu.make_async_remote_copy(
            src_ref=src, dst_ref=dst, send_sem=ssem.at[next(numbers) % NSEND], recv_sem=rsem,
            device_id=target, device_id_type=MESH,
        )
        sends.append((copy, when))
        if when is None:
            copy.start()
        else:
            pl.when(when)(lambda: copy.start())

    def arrived(dst, rsem, when=None):
        copy = pltpu.make_async_remote_copy(
            src_ref=dst, dst_ref=dst, send_sem=ssem.at[0], recv_sem=rsem,
            device_id={"tp": 1 - c}, device_id_type=MESH,
        )
        if when is None:
            copy.wait_recv()
        else:
            pl.when(when)(lambda: copy.wait_recv())

    up = ((z + 1) % ZN) * YN + y
    down = ((z + ZN - 1) % ZN) * YN + y

    def beside(step):
        return z * YN + (y + step + YN) % YN

    def tell(n, distance):
        pl.semaphore_signal(
            known.at[n], inc=1, device_id={"sp": ((z + distance) % ZN) * YN + y}, device_id_type=MESH
        )

    loaded(0, tok.at[c])
    pl.semaphore_wait(barrier, greeted)
    send(tok.at[c], tok.at[c], tsem, tp=1 - c)
    load(8, (wor_h, wor))
    load(9, (woa_h, woa))

    loaded(1, gain)

    def scale_half(half):
        x = tok[half].astype(F32)
        scaled[half] = (x * gain[half]).astype(BF)
        return jnp.sum(x * x, axis=1, keepdims=True)

    squares = scale_half(c)
    tell(0, 1)
    tell(1, ZN - 1)
    loaded(2, wall.at[own_rows])
    acc[...] = dot(scaled[c], wall[own_rows, :])

    arrived(tok.at[1 - c], tsem)
    squares = squares + scale_half(1 - c)
    inverse = lax.rsqrt(squares / D + EPS)
    loaded(3, wall.at[other_rows, kv_cols])
    kv = (acc[:, 0:256] + dot(scaled[1 - c], wall[other_rows, 0:256])) * inverse
    kbuf[sp] = kv[:, 0:128].astype(BF)
    vbuf[sp] = jnp.transpose(kv[:, 128:256]).astype(BF)

    def slot(row, col):
        return row * YN + col

    def send_block(buf, sem, row, col, to, when):
        s = slot(row, col)
        send(buf.at[s], buf.at[s], sem.at[s], when=when, sp=to)

    goes_down = z <= BACK - 1

    def send_down(buf, sem, at, when):
        send(buf.at[at], buf.at[at], sem.at[at], when=when, sp=down)

    def send_v(row, col, to, kind, when):
        s = slot(row, col)
        send(vbuf.at[s], vbuf.at[s], vsem.at[row, kind], when=when, sp=to)

    def forward_own(buf, sem, col):
        send_block(buf, sem, z, col, up, has_up)
        send_down(buf, sem, slot(z, col), goes_down)

    for step in (1, 3, 2):
        send(kbuf.at[sp], kbuf.at[sp], ksem.at[sp], sp=beside(step))
    send_v(z, y, up, 0, has_up)
    send_v(z, y, down, 0, goes_down)
    forward_own(kbuf, ksem, y)

    def plus(buf, sem, d, col):
        row = jnp.maximum(z - d, 0)
        ok = z >= d
        s = slot(row, col)
        arrived(buf.at[s], sem.at[s], ok)
        if d < FWD:
            send_block(buf, sem, row, col, up, ok & has_up)

    def minus(buf, sem, e, col):
        row = (z + e) % ZN
        ok = row <= BACK - 1
        s = slot(row, col)
        arrived(buf.at[s], sem.at[s], ok)
        if e < BACK:
            send_down(buf, sem, s, ok)

    def row_plus(d):
        return jnp.maximum(z - d, 0), z >= d

    def row_minus(e):
        row = (z + e) % ZN
        return row, (row <= BACK - 1) & (z > row)

    def spread_v(row, ok, across=False):
        way = 1 - 2 * (row % 2)
        send_v(row, y, beside(way), 2 if across else 1, ok)
        send_v(row, y, beside(-way), 2, ok)
        if across:
            send_v(row, y, beside(2), 2, ok)

    def relay_v(row, ok):
        way = 1 - 2 * (row % 2)
        col = (y - way + YN) % YN
        arrived(vbuf.at[slot(row, col)], vsem.at[row, 1], ok)
        send_v(row, col, beside(way), 2, ok)

    def finish_v(row, ok, across=False):
        arrived(vbuf.at[pl.ds(slot(row, 0), 3 if across else 2)], vsem.at[row, 2], ok)

    def keys_beside():
        for step in (1, 3):
            col = (y + step) % YN
            s = slot(z, col)
            arrived(kbuf.at[s], ksem.at[s])
            forward_own(kbuf, ksem, col)

    def keys_across():
        col = (y + 2) % YN
        s = slot(z, col)
        arrived(kbuf.at[s], ksem.at[s])
        forward_own(kbuf, ksem, col)

    always = z >= 0
    spread_v(z, always)

    loaded(4, wall.at[other_rows, r_cols])
    recur = ((acc[:, 256:768] + dot(scaled[1 - c], wall[other_rows, 256:768])) * inverse).astype(BF)
    rin[...] = recur
    send(rin.at[pl.ds(ROWS - 16, 16)], halo, hsem, when=sp < SP - 1, sp=(sp + 1) % SP)
    xext[pl.ds(8, ROWS), :] = recur.astype(F32)


    def v_plus(d):
        row, ok = row_plus(d)
        arrived(vbuf.at[slot(row, y)], vsem.at[row, 0], ok)
        if d < FWD:
            send_v(row, y, up, 0, ok & has_up)
        spread_v(row, ok, across=d == FWD)

    def v_minus(e):
        row = (z + e) % ZN
        ok = row <= BACK - 1
        arrived(vbuf.at[slot(row, y)], vsem.at[row, 0], ok)
        if e < BACK:
            send_v(row, y, down, 0, ok)
        spread_v(*row_minus(e), across=e == BACK)

    loaded(5, wall.at[other_rows, q_cols])
    small = (
        (cw_h, cw), (wgd_h, wgd), (wgi_h, wgi), (base_h, base), (extra_h, extra), (lam_h, lam),
        (hgain_h, hgain), (ogain_h, ogain),
    )
    for n, pair in enumerate(small):
        load(n, pair)
    query = ((acc[:, 768:1280] + dot(scaled[1 - c], wall[other_rows, 768:1280])) * inverse).astype(BF)
    query = query.astype(F32) * HEAD ** (-0.5)
    qt[...] = jnp.zeros_like(qt)
    for h in range(4):
        turned = jnp.transpose(query[:, h * 128 : (h + 1) * 128]).astype(BF)
        lanes = slice((h % 2) * 128, (h % 2) * 128 + 128)
        qt[h // 2, 0:64, lanes] = turned[0:64]
        qt[2 + h // 2, 64:128, lanes] = turned[64:128]


    def attend(row, ok, steps=(), first_of_all=False, earlier=False):
        def run():
            if steps:
                slots = [slot(row, (y + step) % YN) for step in steps]
                keys = jnp.concatenate([kbuf[s] for s in slots], axis=0)
                values = jnp.concatenate([vbuf[s] for s in slots], axis=1)
            else:
                first = row * YN
                keys = kbuf[pl.ds(first, YN)].reshape(YN * ROWS, 128)
                values = jnp.concatenate([vbuf[first + i] for i in range(YN)], axis=1)
            all_scores = [dot(keys, qt[part]) for part in range(4)]
            for part, scores in enumerate(all_scores):
                if first_of_all:
                    key_at = lax.broadcasted_iota(jnp.int32, scores.shape, 0)
                    query_at = lax.broadcasted_iota(jnp.int32, scores.shape, 1) % ROWS
                    scores = jnp.where(query_at >= key_at, scores, -1e30)
                    new = jnp.max(scores, axis=0, keepdims=True)
                    weights = jnp.exp(scores - new)
                    total[part] = jnp.sum(weights, axis=0, keepdims=True)
                    att[part] = dot(values, weights.astype(BF))
                else:
                    if earlier:
                        scores = jnp.concatenate(
                            [
                                jnp.where((y + step) % YN < y, scores[n * ROWS : n * ROWS + ROWS], -1e30)
                                for n, step in enumerate(steps)
                            ],
                            axis=0,
                        )
                    old = peak[part]
                    new = jnp.maximum(old, jnp.max(scores, axis=0, keepdims=True))
                    weights = jnp.exp(scores - new)
                    fade = jnp.exp(old - new)
                    total[part] = total[part] * fade + jnp.sum(weights, axis=0, keepdims=True)
                    att[part] = att[part] * fade + dot(values, weights.astype(BF))
                peak[part] = new

        if ok is None:
            run()
        else:
            pl.when(ok)(run)

    attend(z, None, steps=(0,), first_of_all=True)
    v_plus(1)
    v_minus(1)
    keys_beside()
    plus(kbuf, ksem, 1, y)
    minus(kbuf, ksem, 1, y)
    relay_v(z, always)
    pl.semaphore_wait(known.at[0], 1)
    pl.semaphore_wait(known.at[1], 1)
    tell(2, 2)
    tell(3, ZN - 2)

    for n, (_, dst) in enumerate(small):
        loaded(n, dst)
    arrived(halo, hsem, sp > 0)
    before = halo[8:16, :].astype(F32)
    xext[pl.ds(0, 8), :] = jnp.where(sp > 0, before, 0.0)
    conv = jnp.zeros((ROWS, 512), F32)
    for k in range(4):
        conv = conv + cw[k : k + 1, :] * xext[pl.ds(5 + k, ROWS), :]
    conv = conv.astype(BF)
    gates[...] = jnp.zeros_like(gates)
    for j in range(4):
        for side in range(2):
            rows = slice(side * 64, side * 64 + 64)
            gates[j, rows, side * 64 : side * 64 + 64] = wgd[2 * j + side]
            gates[j, rows, 128 + side * 64 : 128 + side * 64 + 64] = wgi[2 * j + side]
    lane = lax.broadcasted_iota(jnp.int32, (ROWS, 128), 1)
    line = lax.broadcasted_iota(jnp.int32, (ROWS, 128), 0)
    extra_t = jnp.transpose(extra[...])
    def recur_columns(j):
        cols = slice(j * 128, j * 128 + 128)
        part = conv[:, cols]
        both = dot(part, gates[j])
        decay_gate = jax.nn.sigmoid(both[:, 0:128])
        input_gate = jax.nn.sigmoid(both[:, 128:256])
        added = jnp.where(lane < 64, extra_t[:, 2 * j : 2 * j + 1], extra_t[:, 2 * j + 1 : 2 * j + 2])
        log_decay = -RATE * decay_gate * base[:, cols] - added
        a = jnp.exp(log_decay)
        b = jnp.sqrt(minus_expm1(2.0 * log_decay)) * input_gate * part.astype(F32)
        for shift in (1, 2, 4, 8, 16, 32, 64):
            inside = line >= shift
            a_back = jnp.where(inside, pltpu.roll(a, shift, 0), 1.0)
            b_back = jnp.where(inside, pltpu.roll(b, shift, 0), 0.0)
            b = a * b_back + b
            a = a * a_back
        decs[:, cols] = a
        states[:, cols] = b
        crow[y, 0:1, cols] = a[ROWS - 1 : ROWS]
        crow[y, 1:2, cols] = b[ROWS - 1 : ROWS]


    def key(sign, n, step):
        move = plus if sign > 0 else minus
        return lambda: move(kbuf, ksem, n, (y + step) % YN)

    def row_carry():
        arrived(crow.at[pl.ds(0, YN - 1)], crsem)
        all_a = crow[0, 0:1, :]
        all_s = crow[0, 1:2, :]
        for col in range(1, YN):
            all_s = crow[col, 0:1, :] * all_s + crow[col, 1:2, :]
            all_a = crow[col, 0:1, :] * all_a
        ctot[z, 0:1, :] = all_a
        ctot[z, 1:2, :] = all_s
        pl.semaphore_wait(known.at[2], 1)
        pl.semaphore_wait(known.at[3], 1)
        for distance in range(1, ZN):
            to = ((z + distance) % ZN) * YN + y
            send(ctot.at[z], ctot.at[z], ctsem, sp=to)

    def carries():
        arrived(ctot.at[pl.ds(0, ZN - 1)], ctsem)

    def fold_total(row, s):
        return ctot[row, 0:1, :] * s + ctot[row, 1:2, :]

    def fold_row(col, s):
        return crow[col, 0:1, :] * s + crow[col, 1:2, :]

    def recur_output():
        carry_in = lax.fori_loop(0, z, fold_total, jnp.zeros((1, 512), F32))
        carry_in = lax.fori_loop(0, y, fold_row, carry_in)
        rout[...] = (states[...] + decs[...] * carry_in).astype(BF)
        loaded(8, wor)

    def recur_project(n):
        mbuf[n] = dot(rout[...], wor[:, n * 512 : n * 512 + 512])

    def drain():
        while sends:
            settle(*sends.pop(0))

    def both(n, *steps):
        for step in steps:
            if n <= FWD:
                key(1, n, step)()
            if n <= BACK:
                key(-1, n, step)()

    def relay(n):
        if n < FWD:
            relay_v(*row_plus(n))
        if n < BACK:
            relay_v(*row_minus(n))

    def finish(sign, n):
        row_of, most = (row_plus, FWD) if sign > 0 else (row_minus, BACK)
        finish_v(*row_of(n), across=n == most)
        attend(*row_of(n))

    far = 1 if FWD == 4 else -1

    recur_columns(0)
    recur_columns(1)
    keys_across()
    v_plus(2)
    v_minus(2)
    relay(1)
    recur_columns(2)
    both(2, 0)
    recur_columns(3)
    for step in (1, 3, 2):
        send(crow.at[y], crow.at[y], crsem, sp=beside(step))
    both(1, 1, 3)
    finish_v(z, always)
    attend(z, None, steps=(1, 2, 3), earlier=True)
    both(1, 2)
    v_plus(3)
    v_minus(3)
    relay(2)
    finish(1, 1)
    row_carry()
    both(3, 0)
    both(2, 1, 3)
    finish(-1, 1)
    both(2, 2)
    (v_plus if FWD == 4 else v_minus)(4)
    relay(3)
    finish(1, 2)
    both(3, 1, 3)
    both(4, 0)
    finish(-1, 2)
    both(3, 2)
    finish(-far, 3)
    carries()
    recur_output()
    for n in range(4):
        recur_project(n)
    finish(far, 3)
    both(4, 1, 3)
    both(4, 2)
    while len(sends) > 8:
        settle(*sends.pop(0))
    finish(far, 4)

    pieces = []
    for h in range(4):
        lanes = slice((h % 2) * 128, (h % 2) * 128 + 128)
        first = att[h // 2, :, lanes] / total[h // 2, :, lanes]
        second = att[2 + h // 2, :, lanes] / total[2 + h // 2, :, lanes]
        out = first - lam[0:1, h : h + 1] * second
        out = out * lax.rsqrt(jnp.mean(out * out, axis=0, keepdims=True) + EPS)
        pieces.append((jnp.transpose(out) * hgain[...]).astype(BF))
    attend_out = jnp.concatenate(pieces, axis=1)

    mine = pl.ds(pl.multiple_of(c * 64, 64), 64)
    theirs = pl.ds(pl.multiple_of((1 - c) * 64, 64), 64)
    loaded(9, woa)
    for n in range(4):
        mbuf[n] += dot(attend_out, woa[:, n * 512 : n * 512 + 512])
        mpart[n] = mbuf[n, theirs, :].astype(BF)
        send(mpart.at[n], mrecv.at[n], msem.at[n], tp=1 - c)
    power = jnp.zeros((64, 1), F32)
    for n in range(4):
        arrived(mrecv.at[n], msem.at[n])
        whole = mbuf[n, mine, :] + mrecv[n].astype(F32)
        mbuf[n, mine, :] = whole
        power = power + jnp.sum(whole * whole, axis=1, keepdims=True)
    scale = lax.rsqrt(power / D + EPS)
    for n in range(4):
        cols = slice(n * 512, n * 512 + 512)
        out_h[:, cols] = (mbuf[n, mine, :] * scale * ogain[:, cols]).astype(BF)
    drain()


def body(
    tokens, norm_gain, w_recur_in, conv_weight, w_gate_decay, w_gate_input, decay_base, extra_decay,
    w_query, w_key, w_value, mix_lambda, head_gain, w_out_recur, w_out_attend, out_gain,
):
    any_ = pl.BlockSpec(memory_space=pl.ANY)
    vmem = pltpu.VMEM
    dma = pltpu.SemaphoreType.DMA
    scratch = [
        vmem((2, ROWS, HALF), BF), vmem((2, 1, HALF), F32), vmem((D, 1280), BF), vmem((4, 512), F32),
        vmem((8, 64, 64), BF), vmem((8, 64, 64), BF), vmem((1, 512), F32), vmem((8, ROWS), F32),
        vmem((1, 4), F32), vmem((1, 128), F32),
        vmem((512, D), BF), vmem((512, D), BF), vmem((1, D), F32),
        vmem((2, ROWS, HALF), BF), vmem((ROWS, 1280), F32),
        vmem((SP, ROWS, 128), BF), vmem((SP, 128, ROWS), BF),
        vmem((ROWS, 512), BF), vmem((16, 512), BF), vmem((ROWS + 8, 512), F32),
        vmem((4, 128, 256), BF), vmem((4, 128, 256), F32), vmem((4, 1, 256), F32), vmem((4, 1, 256), F32),
        vmem((4, 128, 256), BF),
        vmem((YN, 2, 512), F32), vmem((ZN, 2, 512), F32), vmem((ROWS, 512), F32), vmem((ROWS, 512), F32),
        vmem((4, ROWS, 512), F32), vmem((4, 64, 512), BF), vmem((4, 64, 512), BF), vmem((ROWS, 512), BF),
        dma((10,)), dma((NSEND,)), dma, dma((SP,)), dma((ZN, 3)), dma, dma, dma, dma((4,)),
        pltpu.SemaphoreType.REGULAR((4,)),
    ]
    return pl.pallas_call(
        kernel,
        out_shape=pltpu.VMEM((64, D), BF),
        in_specs=[any_] * 16,
        out_specs=pl.BlockSpec(memory_space=pltpu.VMEM),
        scratch_shapes=scratch,
        compiler_params=pltpu.CompilerParams(
            collective_id=0, has_side_effects=True, vmem_limit_bytes=60 * 1024 * 1024
        ),
        name="layer",
    )(
        tokens, norm_gain.reshape(2, 1, HALF), w_recur_in, conv_weight, w_gate_decay, w_gate_input,
        decay_base.reshape(1, -1), extra_decay.T, w_query, w_key, w_value, mix_lambda.reshape(1, -1),
        head_gain.reshape(1, -1), w_out_recur, w_out_attend, out_gain.reshape(1, -1),
    )


def solution(mesh):
    in_specs = (
        P(("fs", "sp"), "tp"),
        P(),
        P(None, "tp"),
        P(None, "tp"),
        P("tp", None, None),
        P("tp", None, None),
        P("tp"),
        P(("fs", "sp"), "tp"),
        P(None, "tp"),
        P(None, "tp"),
        P(None, "tp"),
        P("tp"),
        P(),
        P("tp", None),
        P("tp", None),
        P(),
    )
    out_specs = P(("fs", "sp", "tp"), None)
    return jax.shard_map(body, mesh=mesh, in_specs=in_specs, out_specs=out_specs, check_vma=False)
```

```python
import itertools

import jax
import jax.numpy as jnp
from jax import lax
from jax.experimental import pallas as pl
from jax.experimental.pallas import tpu as pltpu
from jax.sharding import PartitionSpec as P

MESH = pl.DeviceIdType.MESH
BF = jnp.bfloat16
F32 = jnp.float32

D = 2048
HALF = 1024
HEAD = 64
ROWS = 128
ZN = 8
YN = 4
SP = ZN * YN
RATE = 8.0
EPS = 1e-06
FWD = 4
STRAIGHT_UP = (1, 2, 4)
STRAIGHT_DOWN = (3,)
BACK = 3
NSEND = 28


def dot(a, b):
    return jnp.dot(a, b, preferred_element_type=F32)


def minus_expm1(x):
    series = 1.0 + x * (
        1 / 2 + x * (1 / 6 + x * (1 / 24 + x * (1 / 120 + x * (1 / 720 + x * (1 / 5040 + x / 40320)))))
    )
    return jnp.where(x > -0.5, -x * series, 1.0 - jnp.exp(x))


def kernel(
    tok_h, gain_h, wr_h, cw_h, wgd_h, wgi_h, base_h, extra_h, wq_h, wk_h, wv_h, lam_h, hgain_h,
    wor_h, woa_h, ogain_h, out_h,
    tok, gain, wall, cw, wgd, wgi, base, extra, lam, hgain, wor, woa, ogain,
    scaled, acc, kbuf, vbuf, rin, halo, xext, qt, att, peak, total, gates,
    crow, ctot, decs, states, mbuf, mrecv, mpart, rout,
    lsem, ssem, tsem, ksem, vsem, hsem, crsem, ctsem, msem, known,
):
    sp = lax.axis_index("sp")
    c = lax.axis_index("tp")
    z = sp // YN
    y = sp % YN

    def load(n, *pairs):
        for src, dst in pairs:
            pltpu.make_async_copy(src, dst, lsem.at[n]).start()

    def loaded(n, dst):
        pltpu.make_async_copy(dst, dst, lsem.at[n]).wait()

    own_rows = pl.ds(pl.multiple_of(c * HALF, HALF), HALF)
    other_rows = pl.ds(pl.multiple_of((1 - c) * HALF, HALF), HALF)
    kv_cols, r_cols, q_cols = pl.ds(0, 256), pl.ds(256, 512), pl.ds(768, 512)
    load(0, (tok_h, tok.at[c]))
    load(1, (gain_h, gain))

    def load_kv(n, rows):
        load(n, (wk_h.at[rows], wall.at[rows, pl.ds(0, 128)]), (wv_h.at[rows], wall.at[rows, pl.ds(128, 128)]))

    load_kv(2, own_rows)
    load(2, (wr_h.at[own_rows], wall.at[own_rows, r_cols]), (wq_h.at[own_rows], wall.at[own_rows, q_cols]))
    load_kv(3, other_rows)
    load(4, (wr_h.at[other_rows], wall.at[other_rows, r_cols]))
    load(5, (wq_h.at[other_rows], wall.at[other_rows, q_cols]))

    barrier = pltpu.get_barrier_semaphore()
    pl.semaphore_signal(barrier, inc=1, device_id={"tp": 1 - c}, device_id_type=MESH)
    for step in (1, 2, 3):
        pl.semaphore_signal(
            barrier, inc=1, device_id={"sp": z * YN + (y + step) % YN}, device_id_type=MESH
        )
    has_up = z < ZN - 1
    has_down = z > 0
    around = (z == 0) | (z == ZN - 1)
    corner_up = (y == YN - 1) & has_up
    corner_down = (y == 0) & has_down
    greeted = 4
    for when, target in (
        (has_up, (z + 1) * YN + y), (has_down, (z - 1) * YN + y), (around, (ZN - 1 - z) * YN + y),
        (corner_up, sp + 1), (corner_down, sp - 1),
    ):
        near = jnp.where(when, target, sp)

        @pl.when(when)
        def _():
            pl.semaphore_signal(barrier, inc=1, device_id={"sp": near}, device_id_type=MESH)

        greeted = greeted + when.astype(jnp.int32)

    sends = []
    numbers = itertools.count()

    def settle(copy, when):
        if when is None:
            copy.wait_send()
        else:
            pl.when(when)(lambda: copy.wait_send())

    def send(src, dst, rsem, when=None, **target):
        if len(sends) == NSEND:
            settle(*sends.pop(0))
        copy = pltpu.make_async_remote_copy(
            src_ref=src, dst_ref=dst, send_sem=ssem.at[next(numbers) % NSEND], recv_sem=rsem,
            device_id=target, device_id_type=MESH,
        )
        sends.append((copy, when))
        if when is None:
            copy.start()
        else:
            pl.when(when)(lambda: copy.start())

    def arrived(dst, rsem, when=None):
        copy = pltpu.make_async_remote_copy(
            src_ref=dst, dst_ref=dst, send_sem=ssem.at[0], recv_sem=rsem,
            device_id={"tp": 1 - c}, device_id_type=MESH,
        )
        if when is None:
            copy.wait_recv()
        else:
            pl.when(when)(lambda: copy.wait_recv())

    up = ((z + 1) % ZN) * YN + y
    down = ((z + ZN - 1) % ZN) * YN + y

    def beside(step):
        return z * YN + (y + step + YN) % YN

    def tell(n, distance):
        pl.semaphore_signal(
            known.at[n], inc=1, device_id={"sp": ((z + distance) % ZN) * YN + y}, device_id_type=MESH
        )

    loaded(0, tok.at[c])
    pl.semaphore_wait(barrier, greeted)
    send(tok.at[c], tok.at[c], tsem, tp=1 - c)
    load(8, (wor_h, wor))
    load(9, (woa_h, woa))

    loaded(1, gain)

    def scale_half(half):
        x = tok[half].astype(F32)
        scaled[half] = (x * gain[half]).astype(BF)
        return jnp.sum(x * x, axis=1, keepdims=True)

    squares = scale_half(c)
    tell(0, 1)
    tell(1, ZN - 1)
    loaded(2, wall.at[own_rows])
    acc[...] = dot(scaled[c], wall[own_rows, :])

    arrived(tok.at[1 - c], tsem)
    squares = squares + scale_half(1 - c)
    inverse = lax.rsqrt(squares / D + EPS)
    loaded(3, wall.at[other_rows, kv_cols])
    kv = (acc[:, 0:256] + dot(scaled[1 - c], wall[other_rows, 0:256])) * inverse
    kbuf[sp] = kv[:, 0:128].astype(BF)
    vbuf[sp] = jnp.transpose(kv[:, 128:256]).astype(BF)

    def slot(row, col):
        return row * YN + col

    def send_block(buf, sem, row, col, to, when):
        s = slot(row, col)
        send(buf.at[s], buf.at[s], sem.at[s], when=when, sp=to)

    goes_down = z <= BACK - 1

    def send_down(buf, sem, at, when):
        send(buf.at[at], buf.at[at], sem.at[at], when=when, sp=down)

    def send_v(row, col, to, kind, when):
        s = slot(row, col)
        send(vbuf.at[s], vbuf.at[s], vsem.at[row, kind], when=when, sp=to)

    def forward_own(buf, sem, col):
        send_block(buf, sem, z, col, up, has_up)
        send_down(buf, sem, slot(z, col), goes_down)

    for step in (1, 3, 2):
        send(kbuf.at[sp], kbuf.at[sp], ksem.at[sp], sp=beside(step))
    send_v(z, y, up, 0, has_up)
    send_v(z, y, down, 0, goes_down)
    forward_own(kbuf, ksem, y)

    def plus(buf, sem, d, col):
        row = jnp.maximum(z - d, 0)
        ok = z >= d
        s = slot(row, col)
        arrived(buf.at[s], sem.at[s], ok)
        if d < FWD:
            send_block(buf, sem, row, col, up, ok & has_up)

    def minus(buf, sem, e, col):
        row = (z + e) % ZN
        ok = row <= BACK - 1
        s = slot(row, col)
        arrived(buf.at[s], sem.at[s], ok)
        if e < BACK:
            send_down(buf, sem, s, ok)

    def row_plus(d):
        return jnp.maximum(z - d, 0), z >= d

    def row_minus(e):
        row = (z + e) % ZN
        return row, (row <= BACK - 1) & (z > row)

    def spread_v(row, ok, across=False):
        way = 1 - 2 * (row % 2)
        send_v(row, y, beside(way), 2 if across else 1, ok)
        send_v(row, y, beside(-way), 2, ok)
        if across:
            send_v(row, y, beside(2), 2, ok)

    def relay_v(row, ok):
        way = 1 - 2 * (row % 2)
        col = (y - way + YN) % YN
        arrived(vbuf.at[slot(row, col)], vsem.at[row, 1], ok)
        send_v(row, col, beside(way), 2, ok)

    def finish_v(row, ok, across=False):
        arrived(vbuf.at[pl.ds(slot(row, 0), 3 if across else 2)], vsem.at[row, 2], ok)

    def keys_beside():
        for step in (1, 3):
            col = (y + step) % YN
            s = slot(z, col)
            arrived(kbuf.at[s], ksem.at[s])
            forward_own(kbuf, ksem, col)

    def keys_across():
        col = (y + 2) % YN
        s = slot(z, col)
        arrived(kbuf.at[s], ksem.at[s])
        forward_own(kbuf, ksem, col)

    always = z >= 0
    spread_v(z, always)

    loaded(4, wall.at[other_rows, r_cols])
    recur = ((acc[:, 256:768] + dot(scaled[1 - c], wall[other_rows, 256:768])) * inverse).astype(BF)
    rin[...] = recur
    send(rin.at[pl.ds(ROWS - 16, 16)], halo, hsem, when=sp < SP - 1, sp=(sp + 1) % SP)
    xext[pl.ds(8, ROWS), :] = recur.astype(F32)


    def v_plus(d):
        row, ok = row_plus(d)
        arrived(vbuf.at[slot(row, y)], vsem.at[row, 0], ok)
        if d < FWD:
            send_v(row, y, up, 0, ok & has_up)
        spread_v(row, ok, across=d in STRAIGHT_UP)

    def v_minus(e):
        row = (z + e) % ZN
        ok = row <= BACK - 1
        arrived(vbuf.at[slot(row, y)], vsem.at[row, 0], ok)
        if e < BACK:
            send_v(row, y, down, 0, ok)
        spread_v(*row_minus(e), across=e in STRAIGHT_DOWN)

    loaded(5, wall.at[other_rows, q_cols])
    small = (
        (cw_h, cw), (wgd_h, wgd), (wgi_h, wgi), (base_h, base), (extra_h, extra), (lam_h, lam),
        (hgain_h, hgain), (ogain_h, ogain),
    )
    for n, pair in enumerate(small):
        load(n, pair)
    query = ((acc[:, 768:1280] + dot(scaled[1 - c], wall[other_rows, 768:1280])) * inverse).astype(BF)
    query = query.astype(F32) * HEAD ** (-0.5)
    qt[...] = jnp.zeros_like(qt)
    for h in range(4):
        turned = jnp.transpose(query[:, h * 128 : (h + 1) * 128]).astype(BF)
        lanes = slice((h % 2) * 128, (h % 2) * 128 + 128)
        qt[h // 2, 0:64, lanes] = turned[0:64]
        qt[2 + h // 2, 64:128, lanes] = turned[64:128]


    def attend(row, ok, steps=(), first_of_all=False, earlier=False):
        def run():
            if steps:
                slots = [slot(row, (y + step) % YN) for step in steps]
                keys = jnp.concatenate([kbuf[s] for s in slots], axis=0)
                values = jnp.concatenate([vbuf[s] for s in slots], axis=1)
            else:
                first = row * YN
                keys = kbuf[pl.ds(first, YN)].reshape(YN * ROWS, 128)
                values = jnp.concatenate([vbuf[first + i] for i in range(YN)], axis=1)
            all_scores = [dot(keys, qt[part]) for part in range(4)]
            for part, scores in enumerate(all_scores):
                if first_of_all:
                    key_at = lax.broadcasted_iota(jnp.int32, scores.shape, 0)
                    query_at = lax.broadcasted_iota(jnp.int32, scores.shape, 1) % ROWS
                    scores = jnp.where(query_at >= key_at, scores, -1e30)
                    new = jnp.max(scores, axis=0, keepdims=True)
                    weights = jnp.exp(scores - new)
                    total[part] = jnp.sum(weights, axis=0, keepdims=True)
                    att[part] = dot(values, weights.astype(BF))
                else:
                    if earlier:
                        scores = jnp.concatenate(
                            [
                                jnp.where((y + step) % YN < y, scores[n * ROWS : n * ROWS + ROWS], -1e30)
                                for n, step in enumerate(steps)
                            ],
                            axis=0,
                        )
                    old = peak[part]
                    new = jnp.maximum(old, jnp.max(scores, axis=0, keepdims=True))
                    weights = jnp.exp(scores - new)
                    fade = jnp.exp(old - new)
                    total[part] = total[part] * fade + jnp.sum(weights, axis=0, keepdims=True)
                    att[part] = att[part] * fade + dot(values, weights.astype(BF))
                peak[part] = new

        if ok is None:
            run()
        else:
            pl.when(ok)(run)

    attend(z, None, steps=(0,), first_of_all=True)
    v_plus(1)
    v_minus(1)
    keys_beside()
    plus(kbuf, ksem, 1, y)
    minus(kbuf, ksem, 1, y)
    relay_v(z, always)
    pl.semaphore_wait(known.at[0], 1)
    pl.semaphore_wait(known.at[1], 1)
    tell(2, 2)
    tell(3, ZN - 2)

    for n, (_, dst) in enumerate(small):
        loaded(n, dst)
    arrived(halo, hsem, sp > 0)
    before = halo[8:16, :].astype(F32)
    xext[pl.ds(0, 8), :] = jnp.where(sp > 0, before, 0.0)
    conv = jnp.zeros((ROWS, 512), F32)
    for k in range(4):
        conv = conv + cw[k : k + 1, :] * xext[pl.ds(5 + k, ROWS), :]
    conv = conv.astype(BF)
    gates[...] = jnp.zeros_like(gates)
    for j in range(4):
        for side in range(2):
            rows = slice(side * 64, side * 64 + 64)
            gates[j, rows, side * 64 : side * 64 + 64] = wgd[2 * j + side]
            gates[j, rows, 128 + side * 64 : 128 + side * 64 + 64] = wgi[2 * j + side]
    lane = lax.broadcasted_iota(jnp.int32, (ROWS, 128), 1)
    line = lax.broadcasted_iota(jnp.int32, (ROWS, 128), 0)
    extra_t = jnp.transpose(extra[...])
    def recur_columns(j):
        cols = slice(j * 128, j * 128 + 128)
        part = conv[:, cols]
        both = dot(part, gates[j])
        decay_gate = jax.nn.sigmoid(both[:, 0:128])
        input_gate = jax.nn.sigmoid(both[:, 128:256])
        added = jnp.where(lane < 64, extra_t[:, 2 * j : 2 * j + 1], extra_t[:, 2 * j + 1 : 2 * j + 2])
        log_decay = -RATE * decay_gate * base[:, cols] - added
        a = jnp.exp(log_decay)
        b = jnp.sqrt(minus_expm1(2.0 * log_decay)) * input_gate * part.astype(F32)
        for shift in (1, 2, 4, 8, 16, 32, 64):
            inside = line >= shift
            a_back = jnp.where(inside, pltpu.roll(a, shift, 0), 1.0)
            b_back = jnp.where(inside, pltpu.roll(b, shift, 0), 0.0)
            b = a * b_back + b
            a = a * a_back
        decs[:, cols] = a
        states[:, cols] = b
        crow[y, 0:1, cols] = a[ROWS - 1 : ROWS]
        crow[y, 1:2, cols] = b[ROWS - 1 : ROWS]


    def key(sign, n, step):
        move = plus if sign > 0 else minus
        return lambda: move(kbuf, ksem, n, (y + step) % YN)

    def row_carry():
        arrived(crow.at[pl.ds(0, YN - 1)], crsem)
        all_a = crow[0, 0:1, :]
        all_s = crow[0, 1:2, :]
        for col in range(1, YN):
            all_s = crow[col, 0:1, :] * all_s + crow[col, 1:2, :]
            all_a = crow[col, 0:1, :] * all_a
        ctot[z, 0:1, :] = all_a
        ctot[z, 1:2, :] = all_s
        pl.semaphore_wait(known.at[2], 1)
        pl.semaphore_wait(known.at[3], 1)
        for distance in range(1, ZN):
            to = ((z + distance) % ZN) * YN + y
            send(ctot.at[z], ctot.at[z], ctsem.at[jnp.minimum(z, ZN - 2)], when=z + distance < ZN, sp=to)

    def carries():
        for row in range(ZN - 1):
            arrived(ctot.at[row], ctsem.at[row], row < z)

    def fold_total(row, s):
        return ctot[row, 0:1, :] * s + ctot[row, 1:2, :]

    def fold_row(col, s):
        return crow[col, 0:1, :] * s + crow[col, 1:2, :]

    def recur_output():
        carry_in = lax.fori_loop(0, z, fold_total, jnp.zeros((1, 512), F32))
        carry_in = lax.fori_loop(0, y, fold_row, carry_in)
        rout[...] = (states[...] + decs[...] * carry_in).astype(BF)
        loaded(8, wor)

    def recur_project(n):
        mbuf[n] = dot(rout[...], wor[:, n * 512 : n * 512 + 512])

    def drain():
        while sends:
            settle(*sends.pop(0))

    def both(n, *steps):
        for step in steps:
            if n <= FWD:
                key(1, n, step)()
            if n <= BACK:
                key(-1, n, step)()

    def relay(n):
        if n not in STRAIGHT_UP:
            relay_v(*row_plus(n))
        if n not in STRAIGHT_DOWN:
            relay_v(*row_minus(n))

    def finish(sign, n):
        row_of, straight = (row_plus, STRAIGHT_UP) if sign > 0 else (row_minus, STRAIGHT_DOWN)
        finish_v(*row_of(n), across=n in straight)
        attend(*row_of(n))

    far = 1 if FWD == 4 else -1

    recur_columns(0)
    recur_columns(1)
    keys_across()
    v_plus(2)
    v_minus(2)
    recur_columns(2)
    relay(1)
    recur_columns(3)
    for step in (1, 3, 2):
        send(crow.at[y], crow.at[y], crsem, sp=beside(step))
    both(1, 1, 3)
    finish_v(z, always)
    attend(z, None, steps=(1, 2, 3), earlier=True)
    both(2, 0)
    both(1, 2)
    v_plus(3)
    v_minus(3)
    relay(2)
    finish(1, 1)
    row_carry()
    both(3, 0)
    both(2, 1, 3)
    finish(-1, 1)
    both(2, 2)
    (v_plus if FWD == 4 else v_minus)(4)
    relay(3)
    finish(1, 2)
    both(3, 1, 3)
    both(4, 0)
    finish(-1, 2)
    both(3, 2)
    finish(-far, 3)
    carries()
    recur_output()
    for n in range(4):
        recur_project(n)
    finish(far, 3)
    both(4, 1, 3)
    both(4, 2)
    while len(sends) > 8:
        settle(*sends.pop(0))
    finish(far, 4)

    pieces = []
    for h in range(4):
        lanes = slice((h % 2) * 128, (h % 2) * 128 + 128)
        first = att[h // 2, :, lanes] / total[h // 2, :, lanes]
        second = att[2 + h // 2, :, lanes] / total[2 + h // 2, :, lanes]
        out = first - lam[0:1, h : h + 1] * second
        out = out * lax.rsqrt(jnp.mean(out * out, axis=0, keepdims=True) + EPS)
        pieces.append((jnp.transpose(out) * hgain[...]).astype(BF))
    attend_out = jnp.concatenate(pieces, axis=1)

    mine = pl.ds(pl.multiple_of(c * 64, 64), 64)
    theirs = pl.ds(pl.multiple_of((1 - c) * 64, 64), 64)
    loaded(9, woa)
    for n in range(4):
        mbuf[n] += dot(attend_out, woa[:, n * 512 : n * 512 + 512])
        mpart[n] = mbuf[n, theirs, :].astype(BF)
        send(mpart.at[n], mrecv.at[n], msem.at[n], tp=1 - c)
    power = jnp.zeros((64, 1), F32)
    for n in range(4):
        arrived(mrecv.at[n], msem.at[n])
        whole = mbuf[n, mine, :] + mrecv[n].astype(F32)
        mbuf[n, mine, :] = whole
        power = power + jnp.sum(whole * whole, axis=1, keepdims=True)
    scale = lax.rsqrt(power / D + EPS)
    for n in range(4):
        cols = slice(n * 512, n * 512 + 512)
        out_h[:, cols] = (mbuf[n, mine, :] * scale * ogain[:, cols]).astype(BF)
    drain()


def body(
    tokens, norm_gain, w_recur_in, conv_weight, w_gate_decay, w_gate_input, decay_base, extra_decay,
    w_query, w_key, w_value, mix_lambda, head_gain, w_out_recur, w_out_attend, out_gain,
):
    any_ = pl.BlockSpec(memory_space=pl.ANY)
    vmem = pltpu.VMEM
    dma = pltpu.SemaphoreType.DMA
    scratch = [
        vmem((2, ROWS, HALF), BF), vmem((2, 1, HALF), F32), vmem((D, 1280), BF), vmem((4, 512), F32),
        vmem((8, 64, 64), BF), vmem((8, 64, 64), BF), vmem((1, 512), F32), vmem((8, ROWS), F32),
        vmem((1, 4), F32), vmem((1, 128), F32),
        vmem((512, D), BF), vmem((512, D), BF), vmem((1, D), F32),
        vmem((2, ROWS, HALF), BF), vmem((ROWS, 1280), F32),
        vmem((SP, ROWS, 128), BF), vmem((SP, 128, ROWS), BF),
        vmem((ROWS, 512), BF), vmem((16, 512), BF), vmem((ROWS + 8, 512), F32),
        vmem((4, 128, 256), BF), vmem((4, 128, 256), F32), vmem((4, 1, 256), F32), vmem((4, 1, 256), F32),
        vmem((4, 128, 256), BF),
        vmem((YN, 2, 512), F32), vmem((ZN, 2, 512), F32), vmem((ROWS, 512), F32), vmem((ROWS, 512), F32),
        vmem((4, ROWS, 512), F32), vmem((4, 64, 512), BF), vmem((4, 64, 512), BF), vmem((ROWS, 512), BF),
        dma((10,)), dma((NSEND,)), dma, dma((SP,)), dma((ZN, 3)), dma, dma, dma((ZN - 1,)), dma((4,)),
        pltpu.SemaphoreType.REGULAR((4,)),
    ]
    return pl.pallas_call(
        kernel,
        out_shape=pltpu.VMEM((64, D), BF),
        in_specs=[any_] * 16,
        out_specs=pl.BlockSpec(memory_space=pltpu.VMEM),
        scratch_shapes=scratch,
        compiler_params=pltpu.CompilerParams(
            collective_id=0, has_side_effects=True, vmem_limit_bytes=60 * 1024 * 1024
        ),
        name="layer",
    )(
        tokens, norm_gain.reshape(2, 1, HALF), w_recur_in, conv_weight, w_gate_decay, w_gate_input,
        decay_base.reshape(1, -1), extra_decay.T, w_query, w_key, w_value, mix_lambda.reshape(1, -1),
        head_gain.reshape(1, -1), w_out_recur, w_out_attend, out_gain.reshape(1, -1),
    )


def solution(mesh):
    in_specs = (
        P(("fs", "sp"), "tp"),
        P(),
        P(None, "tp"),
        P(None, "tp"),
        P("tp", None, None),
        P("tp", None, None),
        P("tp"),
        P(("fs", "sp"), "tp"),
        P(None, "tp"),
        P(None, "tp"),
        P(None, "tp"),
        P("tp"),
        P(),
        P("tp", None),
        P("tp", None),
        P(),
    )
    out_specs = P(("fs", "sp", "tp"), None)
    return jax.shard_map(body, mesh=mesh, in_specs=in_specs, out_specs=out_specs, check_vma=False)
```
